128 devices in a mesh: sp: 16 (over z, x), dp: 8 (over y, core).
Axes of the slice: x: 4, y: 4, z: 4, core: 2. Of those that a mesh axis runs over, the one named last changes fastest.
Arguments:
- resid: bfloat16 [8, 2048, 2048], P('dp', 'sp'), may hold values from -6 to 6
- queries: bfloat16 [8, 2048, 2048], P('dp', 'sp'), may hold values from -7 to 7
- keys: bfloat16 [8, 2048, 2048], P('dp', 'sp'), may hold values from -7 to 7
- values: bfloat16 [8, 2048, 2048], P('dp', 'sp'), may hold values from -6 to 6
- forget_cache: float32 [8, 32, 2048], P('dp', 'sp'), may hold values from -259 to 0, as said below
- query_gain: float32 [64], replicated, may hold values from 0.5 to 8
- key_gain: float32 [64], replicated, may hold values from 0.5 to 8
- out_weight: bfloat16 [2048, 2048], P(None, 'dp'), may hold values from -0.125 to 0.125
- norm_gain: float32 [2048], replicated, may hold values from 0.1 to 1.9
- routes: int32 [8, 2048, 2], P('dp', 'sp'), may hold values from 0 to 127, all different within a row; in each aligned block of 128 rows (0 to 127, 128 to 255, ..., all dimensions but the last counted through in order) at most 4 rows name the same one
- group_weight: float32 [8, 2048], P('dp', 'sp'), may hold values from 0.2 to 1
- inner_share: float32 [8, 2048, 2], P('dp', 'sp'), may hold values from 0.1 to 1
- expert_gate: bfloat16 [128, 2048, 1024], P(('sp', 'dp')), may hold values from -0.125 to 0.125
- expert_up: bfloat16 [128, 2048, 1024], P(('sp', 'dp')), may hold values from -0.125 to 0.125
- expert_down: bfloat16 [128, 1024, 2048], P(('sp', 'dp')), may hold values from -0.1875 to 0.1875
Outputs:
- layer_out: bfloat16 [8, 2048, 2048], P('dp', 'sp')
The draws below stay inside these ranges and needn't reach their ends.
Inputs may be any that keep to these rules, and one draw needn't show every extreme that they name: `routes`: each row names 2 different experts; the rows of one device name one expert at most 4 times, a bound that some block reaches. `forget_cache`: along positions each head's values never rise.
All inputs are finite; a program needn't handle non-finite values.
Results may differ from the reference program's by a relative error of at most 0.0095.
The reference program's roundings to bfloat16 on the way count: a program that leaves them out, or rounds other values in their place, can miss the bound.
Values may be sent and summed in bfloat16 or wider, within the bound.
A program may use at most 128 MiB of HBM per device.

```python
import math
import jax
import jax.numpy as jnp
import numpy as np
from jax import lax

D = 2048
HEAD_COUNT = 32
HD = 64
FF = 1024
TOPK = 2
TOK_DEV = 128
SEQUENCE_COUNT = 8
SEQUENCE_LENGTH = 2048
EXPERTS = 128
CAP = 4


def paired_rows(key):
    base = jax.random.fold_in(key, 7)
    key_q, key_k = jax.random.split(base, 2)
    shape = (SEQUENCE_COUNT, SEQUENCE_LENGTH, HEAD_COUNT * HD)
    key_rows = jax.random.truncated_normal(key_k, -6.0, 6.0, shape, jnp.float32)
    query_rows = jax.random.truncated_normal(key_q, -6.0, 6.0, shape, jnp.float32)
    return (query_rows, key_rows)


def draw_queries(key, part):
    return paired_rows(key)[0].astype(jnp.bfloat16)


def draw_keys(key, part):
    return paired_rows(key)[1].astype(jnp.bfloat16)


def draw_query_gain(key, part):
    sub = jax.random.fold_in(key, 11)
    return jax.random.uniform(sub, (HD,), jnp.float32, 0.5, 1.5)


def draw_key_gain(key, part):
    sub = jax.random.fold_in(key, 13)
    return jax.random.uniform(sub, (HD,), jnp.float32, 0.5, 1.5)


def draw_forget_cache(key, part):
    random_keys = jax.random.split(jax.random.fold_in(key, 17), 7)
    order = jax.random.permutation(random_keys[0], HEAD_COUNT)
    slow = order < HEAD_COUNT // 2
    total = jax.random.uniform(random_keys[1], (SEQUENCE_COUNT, HEAD_COUNT), jnp.float32, 0.3, 1.0)
    fast_span = jax.random.uniform(random_keys[2], (SEQUENCE_COUNT, HEAD_COUNT), jnp.float32, 30.0, 100.0)
    rate = jnp.where(slow[None, :], total / SEQUENCE_LENGTH, 1.0 / fast_span)
    blocks = SEQUENCE_LENGTH // TOK_DEV
    factor = jnp.exp(jax.random.uniform(random_keys[3], (SEQUENCE_COUNT, HEAD_COUNT, blocks), jnp.float32, -0.693, 0.693))
    factor = jnp.repeat(factor, TOK_DEV, axis=2)
    rough = jax.random.uniform(random_keys[4], (SEQUENCE_COUNT, HEAD_COUNT, SEQUENCE_LENGTH), jnp.float32, 0.3, 1.7)
    baseline_level = -rate[:, :, None] * factor * rough
    spike_location = jax.random.randint(random_keys[5], (SEQUENCE_COUNT, HEAD_COUNT, 3), 0, SEQUENCE_LENGTH)
    spike_dropped = jnp.log(jax.random.uniform(random_keys[6], (SEQUENCE_COUNT, HEAD_COUNT, 3), jnp.float32, 0.5, 0.8))
    token_offset = jnp.arange(SEQUENCE_LENGTH, dtype=jnp.int32)
    spike_events = jnp.sum(jnp.where(token_offset[None, None, None, :] == spike_location[..., None], spike_dropped[..., None], 0.0), axis=2)
    return jnp.cumsum(baseline_level + spike_events, axis=2)


def level_of(own_key, dims, cuts, smallest, top_value):
    def one(dim, parts):
        heights = jax.random.uniform(jax.random.fold_in(jax.random.fold_in(own_key, 6), dim), (parts,), jnp.float32, smallest / len(cuts), top_value / len(cuts))
        return jnp.repeat(jnp.exp(heights), dims[dim] // parts).reshape((-1,) + (1,) * (len(dims) - dim - 1))

    level = one(*cuts[0])
    for cut in cuts[1:]:
        level = level * one(*cut)
    return level


def shared_out(key, own, number, rows, count, top, bound, lean):
    ranking = jax.random.permutation(key, count)
    packed, ordinary = portions_of(count, rows * top, bound, lean, True), portions_of(count, rows * top, bound, lean, False)
    places = jnp.arange(count)

    def named(tallies, offset_by):
        used = int((tallies > 0).sum())
        fixed = max(1, used // 4)
        moved = fixed + (places - fixed + offset_by * (used - fixed)) % max(1, count - fixed)
        return jnp.zeros((count,), jnp.int32).at[ranking[jnp.where(places < fixed, places, moved)]].set(jnp.asarray(tallies, jnp.int32))

    tallies = jnp.where(number % 4 == 0, named(packed, number // 4), named(ordinary, number - number // 4 - 1))
    mixed = jax.random.permutation(jax.random.fold_in(own, 3), count)
    source_of, receiver = mixed[0:count // 2 * 2:2], mixed[1:count // 2 * 2:2]
    margin = jnp.minimum(tallies[source_of] - 1, bound - tallies[receiver]) // 2
    margin = jnp.where((source_of == ranking[0]) | (receiver == ranking[0]) | (tallies[receiver] == 0), 0, jnp.maximum(margin, 0))
    moved = jax.random.randint(jax.random.fold_in(own, 4), (count // 2,), 0, 1 << 20) % (margin + 1)
    tallies = tallies.at[source_of].add(-moved).at[receiver].add(moved)
    members = jnp.searchsorted(jnp.cumsum(tallies), jnp.arange(rows * top), side="right").astype(jnp.int32)
    listing = members.reshape(top, rows).T
    listing = listing[jax.random.permutation(jax.random.fold_in(own, 1), rows)]
    offset_by = jax.random.randint(jax.random.fold_in(own, 2), (rows, 1), 0, top)
    return jnp.take_along_axis(listing, (jnp.arange(top)[None, :] + offset_by) % top, axis=1)


def portions_of(number_of, total, limit, lean, full):
    loads = [(1 << 20) // math.isqrt(grade ** lean) + 1 for grade in range(1, number_of + 1)]
    largest = limit if full else min(limit, max(-(-total // number_of), total * loads[0] // sum(loads)))
    least = 1 if total - largest >= number_of - 1 else 0
    counts, surplus = [largest] + [least] * (number_of - 1), total - largest - least * (number_of - 1)
    while surplus > 0:
        free = [i for i in range(1, number_of) if counts[i] < largest] or [i for i in range(1, number_of) if counts[i] < limit]
        pool, remaining = sum([loads[i] for i in free]), surplus
        for i in free:
            extra = min(limit - counts[i], max(1, remaining * loads[i] // pool), surplus)
            counts[i] = counts[i] + extra
            surplus = surplus - extra
    return np.array(counts)


def centred(key, dims, width, limit, shards=(), kind=jnp.bfloat16):
    entries = jax.random.normal(key, dims, jnp.float32) * width
    if len(shards) > 0:
        entries = level_of(key, dims, shards, -0.22, 0.18) * entries
    return jnp.clip(entries, min=-limit, max=limit).astype(kind)


def setup_inputs(seed: int = 0) -> dict:
    key_of = jax.random.split(jax.random.key(seed), 16)
    resid = centred(key_of[0], (SEQUENCE_COUNT, SEQUENCE_LENGTH, D), 1.0, 6.0, ((0, 8), (1, 16)))
    queries = draw_queries(jax.random.fold_in(key_of[15], 71), 0)
    keys = draw_keys(jax.random.fold_in(key_of[15], 71), 0)
    values = centred(key_of[3], (SEQUENCE_COUNT, SEQUENCE_LENGTH, HEAD_COUNT * HD), 1.0, 6.0, ((0, 8), (1, 16)))
    forget_cache = draw_forget_cache(jax.random.fold_in(key_of[15], 71), 0)
    query_gain = draw_query_gain(jax.random.fold_in(key_of[15], 71), 0)
    key_gain = draw_key_gain(jax.random.fold_in(key_of[15], 71), 0)
    out_weight = centred(key_of[7], (HEAD_COUNT * HD, D), (HEAD_COUNT * HD) ** -0.5, 0.125, ((1, 8),))
    norm_gain = jnp.clip(1.0 + 0.18 * jax.random.normal(key_of[8], (D,), jnp.float32), 0.1, 1.9)
    routes_keys = jax.random.split(jax.random.fold_in(key_of[9], 1), SEQUENCE_COUNT * SEQUENCE_LENGTH // TOK_DEV)
    routes_turns = jax.random.permutation(jax.random.fold_in(key_of[9], 3), SEQUENCE_COUNT * SEQUENCE_LENGTH // TOK_DEV)
    routes = jax.vmap(lambda own, number: shared_out(jax.random.fold_in(key_of[9], 2), own, number, TOK_DEV, EXPERTS, TOPK, CAP, 2))(routes_keys, routes_turns).reshape((SEQUENCE_COUNT, SEQUENCE_LENGTH, TOPK))
    group_weight = jnp.clip(jnp.exp(math.log(1.0) - 1.609438 * jax.random.uniform(key_of[10], (SEQUENCE_COUNT, SEQUENCE_LENGTH), jnp.float32) ** level_of(key_of[10], (SEQUENCE_COUNT, SEQUENCE_LENGTH), ((0, 8), (1, 16)), -0.2, 0.2)), 0.2, 1.0)
    inner_share = jnp.clip(jnp.exp(math.log(1.0) - 2.3025851 * jax.random.uniform(key_of[11], (SEQUENCE_COUNT, SEQUENCE_LENGTH, TOPK), jnp.float32) ** level_of(key_of[11], (SEQUENCE_COUNT, SEQUENCE_LENGTH, TOPK), ((0, 8), (1, 16)), -0.2, 0.2)), 0.1, 1.0)
    expert_gate = centred(key_of[12], (EXPERTS, D, FF), D ** -0.5, 0.125, ((0, 128),))
    expert_up = centred(key_of[13], (EXPERTS, D, FF), D ** -0.5, 0.125, ((0, 128),))
    expert_down = centred(key_of[14], (EXPERTS, FF, D), FF ** -0.5, 0.1875, ((0, 128),))
    return dict(resid=resid, queries=queries, keys=keys, values=values, forget_cache=forget_cache, query_gain=query_gain, key_gain=key_gain, out_weight=out_weight, norm_gain=norm_gain, routes=routes, group_weight=group_weight, inner_share=inner_share, expert_gate=expert_gate, expert_up=expert_up, expert_down=expert_down)


EPS = 1e-06

def norm_rows(inputs, gain):
    floats = inputs.astype(jnp.float32)
    scaled = floats * lax.rsqrt(lax.optimization_barrier(jnp.mean(floats * floats, axis=-1, keepdims=True)) + EPS)
    return (scaled * gain.astype(jnp.float32)).astype(jnp.bfloat16)

def head_attention(operands):
    query_rows, key_rows, value_rows, decay = operands
    scores = jnp.dot(query_rows, key_rows.T, preferred_element_type=jnp.float32) * HD ** (-0.5)
    scores = scores + decay[:, None] - decay[None, :]
    token_offset = jnp.arange(query_rows.shape[0], dtype=jnp.int32)
    scores = jnp.where(token_offset[None, :] <= token_offset[:, None], scores, -jnp.inf)
    highest = lax.optimization_barrier(jnp.max(scores, axis=-1, keepdims=True))
    expd = jnp.exp(scores - highest)
    probs = (expd / lax.optimization_barrier(jnp.sum(expd, axis=-1, keepdims=True))).astype(jnp.bfloat16)
    return jnp.dot(probs, value_rows, preferred_element_type=jnp.float32).astype(jnp.bfloat16)

def reference(resid, queries, keys, values, forget_cache, query_gain, key_gain, out_weight, norm_gain, routes, group_weight, inner_share, expert_gate, expert_up, expert_down):

    def sequence_attention(operands):
        seq_q, seq_k, seq_v, seq_c = operands
        query_normed = norm_rows(seq_q.reshape(SEQUENCE_LENGTH, HEAD_COUNT, HD), query_gain).transpose(1, 0, 2)
        key_normed = norm_rows(seq_k.reshape(SEQUENCE_LENGTH, HEAD_COUNT, HD), key_gain).transpose(1, 0, 2)
        value_heads = seq_v.reshape(SEQUENCE_LENGTH, HEAD_COUNT, HD).transpose(1, 0, 2)
        outputs = lax.map(head_attention, (query_normed, key_normed, value_heads, seq_c))
        return outputs.transpose(1, 0, 2).reshape(SEQUENCE_LENGTH, HEAD_COUNT * HD)
    attn = lax.map(sequence_attention, (queries, keys, values, forget_cache))
    projected = jnp.dot(attn.reshape(-1, HEAD_COUNT * HD), out_weight, preferred_element_type=jnp.float32)
    mid = (resid.reshape(-1, D).astype(jnp.float32) + projected).astype(jnp.bfloat16)
    normed = norm_rows(mid, norm_gain)
    shares = inner_share.reshape(-1, TOPK).astype(jnp.float32)
    weights = group_weight.reshape(-1, 1).astype(jnp.float32) * shares / lax.optimization_barrier(jnp.sum(shares, axis=-1, keepdims=True))
    flat_weights = weights.reshape(-1)
    flat_routes = routes.reshape(-1).astype(jnp.int32)
    slot_count = EXPERTS * CAP
    slot_place = jnp.arange(slot_count, dtype=jnp.int32)

    def one_expert(total, expert_index):
        hit = flat_routes == expert_index
        hit_count = jnp.sum(hit.astype(jnp.int32))
        picked = jnp.nonzero(hit, size=slot_count, fill_value=0)[0].astype(jnp.int32)
        live = slot_place < hit_count
        token_index = (picked // TOPK).astype(jnp.int32)
        rows = normed[token_index]
        gate = jnp.dot(rows, expert_gate[expert_index], preferred_element_type=jnp.float32)
        upper = jnp.dot(rows, expert_up[expert_index], preferred_element_type=jnp.float32)
        hidden = (jax.nn.silu(gate) * upper).astype(jnp.bfloat16)
        result = jnp.dot(hidden, expert_down[expert_index], preferred_element_type=jnp.float32).astype(jnp.bfloat16)
        scale = jnp.where(live, flat_weights[picked], jnp.zeros_like(flat_weights[picked]))
        total = total.at[token_index].add(result.astype(jnp.float32) * scale[:, None])
        return (total, None)
    start = jnp.zeros((mid.shape[0], D), jnp.float32)
    mixed, _ = lax.scan(one_expert, start, jnp.arange(EXPERTS, dtype=jnp.int32))
    layer_out = (mid.astype(jnp.float32) + mixed).astype(jnp.bfloat16)
    return layer_out.reshape(SEQUENCE_COUNT, SEQUENCE_LENGTH, D)
```

```python
import functools

import jax
import jax.numpy as jnp
from jax import lax
from jax.experimental import pallas as pl
from jax.experimental.pallas import tpu as pltpu
from jax.sharding import PartitionSpec as P

EPS = 1e-06
MESH = pl.DeviceIdType.MESH
F32 = jnp.float32
BF16 = jnp.bfloat16
D = 2048
HD = 64
FF = 1024
TOK = 128
SEQ = 2048
QB = 256
MULT = 37
SP_MULT = 7


def dot(a, b):
    return jnp.dot(a, b, preferred_element_type=F32)


def drain(ref, sem):
    pltpu.make_async_copy(ref, ref, sem).wait()


def iota(shape, dim):
    return lax.broadcasted_iota(jnp.int32, shape, dim)


def mod(a, n):
    return lax.rem(a, n)


def kernel(
    q_h,
    k_h,
    v_h,
    resid_h,
    ow_h,
    eg_h,
    eu_h,
    ed_h,
    fc_ref,
    qg_ref,
    kg_ref,
    ng_ref,
    routes_ref,
    gw_ref,
    ish_ref,
    out_ref,
    qkv_s,
    qkv_r,
    qh,
    kt,
    ao,
    ar,
    wsrc,
    wr,
    psend,
    precv,
    resid_s,
    disp,
    pick,
    perm,
    wg,
    wu,
    wd,
    send,
    recv,
    ysend,
    ret,
    acc,
    wts,
    loc_sem,
    qkv_send,
    qkv_recv,
    w_send,
    w_near,
    w_far,
    w_part,
    a_send,
    a_recv,
    p_send,
    p_recv,
    d_send,
    d_recv,
    r_send,
    r_recv,
    ready,
):
    sp = lax.axis_index("sp")
    dp = lax.axis_index("dp")
    z, x = sp // 4, mod(sp, 4)
    y, c = dp // 2, mod(dp, 2)
    sign = 1 - 2 * c

    local = []
    for n, (src, dst) in enumerate(
        (
            (k_h, qkv_s.at[0]),
            (q_h, qkv_s.at[1]),
            (v_h, qkv_s.at[2]),
            (ow_h, wsrc),
            (ow_h.at[pl.ds(pl.multiple_of(c * 1024, 1024), 1024)],
             wr.at[:, pl.ds(pl.multiple_of(dp * 256, 256), 256)]),
            (resid_h, resid_s),
        )
    ):
        copy = pltpu.make_async_copy(src, dst, loc_sem.at[n])
        copy.start()
        local.append(copy)
    barrier = pltpu.get_barrier_semaphore()
    for k in range(1, 16):
        pl.semaphore_signal(barrier, inc=1, device_id=(mod(sp + k, 16), dp), device_id_type=MESH)
    for k in range(1, 8):
        pl.semaphore_signal(barrier, inc=1, device_id=(sp, mod(dp + k, 8)), device_id_type=MESH)
    pl.semaphore_wait(barrier, 22)

    def remote(src, dst, ssem, rsem, dev):
        return pltpu.make_async_remote_copy(
            src_ref=src, dst_ref=dst, send_sem=ssem, recv_sem=rsem, device_id=dev, device_id_type=MESH
        )

    my_rows = pl.ds(pl.multiple_of(sp * TOK, TOK), TOK)
    for ten in range(3):
        local[ten].wait()

        def send_qkv(i, _, ten=ten):
            d = mod(SP_MULT * i, 16)
            t = mod(z + sign * (d // 4) + 4, 4) * 4 + mod(x + sign * mod(d, 4) + 4, 4)
            remote(
                qkv_s.at[ten, :, pl.ds(pl.multiple_of(t * 128, 128), 128)],
                qkv_r.at[ten, my_rows, :],
                qkv_send.at[ten],
                qkv_recv.at[ten],
                (t, dp),
            ).start()
            return 0

        lax.fori_loop(1, 16, send_qkv, 0)
        if ten == 0:
            local[3].wait()
            for s, step in enumerate((1, 3)):
                for h in range(2):
                    remote(
                        wsrc.at[pl.ds(1024 * h, 1024)],
                        wr.at[:, pl.ds(pl.multiple_of(dp * 256, 256), 256)],
                        w_send.at[2 * s + h],
                        w_near.at[s],
                        (sp, mod(y + step, 4) * 2 + h),
                    ).start()
            remote(
                wsrc.at[pl.ds(pl.multiple_of((1 - c) * 1024, 1024), 1024)],
                wr.at[:, pl.ds(pl.multiple_of(dp * 256, 256), 256)],
                w_send.at[4],
                w_part,
                (sp, y * 2 + 1 - c),
            ).start()
        qkv_r[ten, my_rows, :] = qkv_s[ten, :, pl.ds(pl.multiple_of(sp * 128, 128), 128)]
    for k in range(1, 8):
        pl.semaphore_signal(ready, inc=1, device_id=(sp, mod(dp + k, 8)), device_id_type=MESH)
    experts = []
    for n, (src, dst) in enumerate(((eg_h, wg), (eu_h, wu), (ed_h, wd))):
        copy = pltpu.make_async_copy(src, dst, loc_sem.at[6 + n])
        copy.start()
        experts.append(copy)

    def expert_of(i):
        d = (MULT * i) & 127
        dz, dx, dy, dc = d & 3, (d >> 2) & 3, (d >> 4) & 3, d >> 6
        ts = ((z + sign * dz + 4) & 3) * 4 + ((x + sign * dx + 4) & 3)
        td = ((y + sign * dy + 4) & 3) * 2 + ((c + dc) & 1)
        return ts * 8 + td

    routes = routes_ref[...]
    r_col = [jnp.broadcast_to(routes[:, k : k + 1].astype(F32), (TOK, 128)) for k in range(2)]
    r_row = [m.T for m in r_col]
    lane = iota((TOK, 128), 1)
    sub = iota((TOK, 128), 0)
    hit_c = [(m == lane.astype(F32)).astype(F32) for m in r_col]
    hit_r = [(m == sub.astype(F32)).astype(F32) for m in r_row]
    lower = (lane < sub).astype(F32).astype(BF16)
    upper = (sub < lane).astype(F32).astype(BF16)
    before_c = dot(lower, (hit_c[0] + hit_c[1]).astype(BF16))
    before_r = dot((hit_r[0] + hit_r[1]).astype(BF16), upper)
    slot_c = [
        4.0 * r_col[k][:, :1] + jnp.sum(before_c * hit_c[k], axis=1, keepdims=True) for k in range(2)
    ]
    slot_r = [
        4.0 * r_row[k][:1, :] + jnp.sum(before_r * hit_r[k], axis=0, keepdims=True) for k in range(2)
    ]
    row = iota((1024, 128), 0)
    row_slot = (4 * expert_of(row >> 3) + (row & 3)).astype(F32)
    row_half = (row >> 2) & 1
    chosen = (row_slot == slot_r[0]) | (row_slot == slot_r[1])
    for g in range(2):
        disp[:, g * 128 : (g + 1) * 128] = jnp.where(chosen & (row_half == g), 1.0, 0.0).astype(BF16)
    col = iota((TOK, 1024), 1)
    col_slot = (4 * expert_of(col >> 3) + (col & 3)).astype(F32)
    col_half = (col >> 2) & 1
    for k in range(2):
        for g in range(2):
            at = (2 * k + g) * 128
            pick[at : at + 128, :] = jnp.where(
                (col_slot == slot_c[k]) & (col_half == g), 1.0, 0.0
            ).astype(BF16)
    shares = ish_ref[...]
    group = jnp.broadcast_to(gw_ref[...], (TOK, 128)).T[:, :1]
    share_sum = shares[:, 0:1] + shares[:, 1:2]
    for k in range(2):
        wts[k] = jnp.broadcast_to(group * shares[:, k : k + 1] / share_sum, (TOK, 128))
    p_o, p_i = iota((256, 256), 0), iota((256, 256), 1)
    perm[0] = jnp.where(
        p_i == 8 * ((p_o >> 2) & 31) + 4 * (p_o >> 7) + (p_o & 3), 1.0, 0.0
    ).astype(BF16)
    perm[1] = jnp.where(
        p_o == 8 * ((p_i >> 2) & 31) + 4 * (p_i >> 7) + (p_i & 3), 1.0, 0.0
    ).astype(BF16)

    def normed_heads(ten, at, size, gain_ref):
        rows = qkv_r[ten, at : at + size, :].astype(F32)
        square = rows * rows
        first = iota((size, 128), 1) < HD
        sum0 = jnp.sum(jnp.where(first, square, 0.0), axis=1, keepdims=True)
        sum1 = jnp.sum(jnp.where(first, 0.0, square), axis=1, keepdims=True)
        factor = jnp.where(
            first, lax.rsqrt(sum0 * (1.0 / HD) + EPS), lax.rsqrt(sum1 * (1.0 / HD) + EPS)
        )
        return (rows * factor * gain_ref[...]).astype(BF16).astype(F32)

    drain(qkv_r.at[0, pl.ds(0, 15 * TOK)], qkv_recv.at[0])
    step = 512
    for at in range(0, SEQ, step):
        turned = normed_heads(0, at, step, kg_ref).T
        sub = iota((128, step), 0)
        for h in range(2):
            bias = fc_ref[h : h + 1, at : at + step]
            high = bias.astype(BF16).astype(F32)
            middle = (bias - high).astype(BF16).astype(F32)
            low = bias - high - middle
            base = 64 * (1 - h)
            extra = jnp.where(
                sub == base, high, jnp.where(sub == base + 1, middle, jnp.where(sub == base + 2, low, 0.0))
            )
            mine = (sub < HD) if h == 0 else (sub >= HD)
            kt[h, :, at : at + step] = jnp.where(mine, turned, extra).astype(BF16)
    drain(qkv_r.at[1, pl.ds(0, 15 * TOK)], qkv_recv.at[1])
    for at in range(0, SEQ, step):
        scaled = normed_heads(1, at, step, qg_ref) * (HD**-0.5)
        lane = iota((step, 128), 1)
        for h in range(2):
            base = 64 * (1 - h)
            mine = (lane < HD) if h == 0 else (lane >= HD)
            extra = jnp.where((lane >= base) & (lane < base + 3), -1.0, 0.0)
            qh[h, at : at + step, :] = jnp.where(mine, scaled, extra).astype(BF16)
    drain(qkv_r.at[2, pl.ds(0, 15 * TOK)], qkv_recv.at[2])

    half = sp // 8
    a_cols = pl.ds(pl.multiple_of(mod(sp, 8) * 128, 128), 128)
    a_rows = pl.ds(pl.multiple_of(c * TOK, TOK), TOK)

    def return_block(t):
        own = jnp.logical_and(sp == t, half == c)

        @pl.when(own)
        def _():
            ar[a_rows, a_cols] = ao[t * TOK : (t + 1) * TOK, :]

        @pl.when(jnp.logical_not(own))
        def _():
            remote(
                ao.at[pl.ds(t * TOK, TOK)], ar.at[a_rows, a_cols], a_send, a_recv, (t, y * 2 + half)
            ).start()

    blocks = SEQ // QB
    tri = iota((QB, QB), 1) <= iota((QB, QB), 0)
    first = iota((QB, 128), 1) < HD
    pending = None
    for n, i in enumerate(reversed(range(blocks))):
        at, keys = i * QB, (i + 1) * QB
        results = []
        for h in range(2):
            query = qh[h, at:keys, :]
            diag = jnp.where(tri, dot(query, kt[h, :, at:keys]), -jnp.inf)
            highest = jnp.max(diag, axis=1, keepdims=True)
            if at:
                past = dot(query, kt[h, :, :at])
                highest = jnp.maximum(highest, jnp.max(past, axis=1, keepdims=True))
            diag = jnp.exp(diag - highest)
            total = jnp.sum(diag, axis=1, keepdims=True)
            result = dot(diag.astype(BF16), qkv_r[2, at:keys, :])
            if at:
                past = jnp.exp(past - highest)
                total = total + jnp.sum(past, axis=1, keepdims=True)
                result = result + dot(past.astype(BF16), qkv_r[2, :at, :])
            results.append(result / total)
        ao[at:keys, :] = jnp.where(first, results[0], results[1]).astype(BF16)
        if pending is not None:
            return_block(2 * pending)
            return_block(2 * pending + 1)
        pending = i
        if n == 3:
            for s, (near, onward) in enumerate(((3, 1), (1, 3))):
                drain(wr.at[:, pl.ds(0, 512)], w_near.at[s])
                part = wr.at[pl.ds(512 * s, 512), pl.ds(pl.multiple_of(mod(y + near, 4) * 512, 512), 512)]
                remote(part, part, w_send.at[5 + s], w_far, (sp, mod(y + onward, 4) * 2 + c)).start()
    return_block(0)
    return_block(1)

    local[4].wait()
    local[5].wait()
    drain(wr.at[:, pl.ds(0, 256)], w_part)
    drain(wr.at[:, pl.ds(0, 512)], w_far)
    own_in = half == c

    @pl.when(own_in)
    def _():
        drain(ao.at[pl.ds(0, 15 * TOK)], a_recv)
        drain(ao.at[pl.ds(0, 15 * TOK)], a_send)

    @pl.when(jnp.logical_not(own_in))
    def _():
        drain(ao.at[pl.ds(0, 16 * TOK)], a_recv)
        drain(ao.at[pl.ds(0, 16 * TOK)], a_send)

    other = ar[pl.ds(pl.multiple_of((1 - c) * TOK, TOK), TOK), :]
    for n in range(4):
        cols = pl.ds(512 * n, 512)
        psend[n] = dot(other, wr[:, cols])
        remote(psend.at[n], precv.at[n], p_send, p_recv, (sp, y * 2 + 1 - c)).start()
    mine = ar[a_rows, :]
    parts = [dot(mine, wr[:, 512 * n : 512 * n + 512]) for n in range(4)]
    drain(precv, p_recv)
    mids = []
    square = None
    for n in range(4):
        cols = slice(512 * n, 512 * n + 512)
        mid = (resid_s[:, cols].astype(F32) + (parts[n] + precv[n])).astype(BF16)
        resid_s[:, cols] = mid
        mid = mid.astype(F32)
        mids.append(mid)
        term = jnp.sum(mid * mid, axis=1, keepdims=True)
        square = term if square is None else square + term
    factor = lax.rsqrt(square * (1.0 / D) + EPS)
    normed = [
        (mids[n] * factor * ng_ref[:, 512 * n : 512 * n + 512]).astype(BF16) for n in range(4)
    ]
    halves = [jnp.concatenate(normed[2 * g : 2 * g + 2], axis=1) for g in range(2)]
    stacked = jnp.concatenate(halves, axis=0)
    for b in range(4):
        send[b * 32 : (b + 1) * 32] = (
            dot(disp[b * 256 : (b + 1) * 256, :], stacked).astype(BF16).reshape(32, 8, 1024)
        )

    pl.semaphore_wait(ready, 7)

    def partner(i, way):
        d = mod(MULT * i, 128)
        dz, dx, dy, dc = mod(d, 4), mod(d // 4, 4), mod(d // 16, 4), d // 64
        ts = mod(z + way * dz + 4, 4) * 4 + mod(x + way * dx + 4, 4)
        td = mod(y + way * dy + 4, 4) * 2 + mod(c + dc, 2)
        return ts, td

    def send_rows(i, _):
        remote(send.at[i], recv.at[i], d_send, d_recv.at[i // 32], partner(i, sign)).start()
        return 0

    lax.fori_loop(1, 128, send_rows, 0)
    recv[0] = send[0]
    for copy in experts:
        copy.wait()

    def wait_block(ref, sem, b):
        @pl.when(b == 0)
        def _():
            drain(ref.at[pl.ds(0, 31)], sem.at[b])

        @pl.when(b > 0)
        def _():
            drain(ref.at[pl.ds(0, 32)], sem.at[b])

    def run_expert(b, _):
        wait_block(recv, d_recv, b)
        at = pl.multiple_of(b * 32, 32)
        rows = recv[pl.ds(at, 32)].reshape(256, 1024)
        rows = dot(perm[0], rows).astype(BF16)
        gate = dot(rows[:128], wg[:1024, :]) + dot(rows[128:], wg[1024:, :])
        up = dot(rows[:128], wu[:1024, :]) + dot(rows[128:], wu[1024:, :])
        hidden = (gate / (1.0 + jnp.exp(-gate)) * up).astype(BF16)
        result = [dot(hidden, wd[:, g * 1024 : (g + 1) * 1024]).astype(BF16) for g in range(2)]
        back = dot(perm[1], jnp.concatenate(result, axis=0)).astype(BF16)
        ysend[pl.ds(at, 32)] = back.reshape(32, 8, 1024)

        def send_back(i, _):
            d = mod(MULT * i, 128)
            src_sign = sign * (1 - 2 * (d // 64))
            remote(ysend.at[i], ret.at[i], r_send, r_recv.at[b], partner(i, -src_sign)).start()
            return 0

        lax.fori_loop(jnp.where(b == 0, 1, b * 32), b * 32 + 32, send_back, 0)

        @pl.when(b == 0)
        def _():
            ret[0] = ysend[0]

        return 0

    lax.fori_loop(0, 4, run_expert, 0)
    acc[...] = jnp.zeros_like(acc)

    def collect(b, _):
        wait_block(ret, r_recv, b)
        rows = ret[pl.ds(pl.multiple_of(b * 32, 32), 32)].reshape(256, 1024)
        acc[...] += dot(pick[:, pl.ds(pl.multiple_of(b * 256, 256), 256)], rows)
        return 0

    lax.fori_loop(0, 4, collect, 0)
    for g in range(2):
        cols = slice(1024 * g, 1024 * g + 1024)
        mixed = wts[0][:, :1] * acc[g * 128 : g * 128 + 128, :]
        mixed = mixed + wts[1][:, :1] * acc[(2 + g) * 128 : (3 + g) * 128, :]
        out_ref[:, cols] = (resid_s[:, cols].astype(F32) + mixed).astype(BF16)

    for ten in range(3):
        drain(qkv_r.at[ten, pl.ds(0, 15 * TOK)], qkv_send.at[ten])
    for n in range(5):
        drain(wr.at[:, pl.ds(0, 256)], w_send.at[n])
    for n in range(5, 7):
        drain(wr.at[:, pl.ds(0, 256)], w_send.at[n])
    drain(precv, p_send)
    drain(recv.at[pl.ds(0, 127)], d_send)
    drain(recv.at[pl.ds(0, 127)], r_send)


def shards(
    resid,
    queries,
    keys,
    values,
    forget_cache,
    query_gain,
    key_gain,
    out_weight,
    norm_gain,
    routes,
    group_weight,
    inner_share,
    expert_gate,
    expert_up,
    expert_down,
):
    any_spec = pl.BlockSpec(memory_space=pl.ANY)
    vmem_spec = pl.BlockSpec(memory_space=pltpu.VMEM)
    vm = pltpu.VMEM
    dma = pltpu.SemaphoreType.DMA
    out = pl.pallas_call(
        kernel,
        out_shape=jax.ShapeDtypeStruct((TOK, D), BF16),
        in_specs=[any_spec] * 8 + [vmem_spec] * 7,
        out_specs=vmem_spec,
        scratch_shapes=[
            vm((3, TOK, D), BF16),
            vm((3, SEQ, 128), BF16),
            vm((2, SEQ, 128), BF16),
            vm((2, 128, SEQ), BF16),
            vm((SEQ, 128), BF16),
            vm((2 * TOK, 1024), BF16),
            vm((D, 256), BF16),
            vm((1024, D), BF16),
            vm((4, TOK, 512), F32),
            vm((4, TOK, 512), F32),
            vm((TOK, D), BF16),
            vm((1024, 256), BF16),
            vm((512, 1024), BF16),
            vm((2, 256, 256), BF16),
            vm((D, FF), BF16),
            vm((D, FF), BF16),
            vm((FF, D), BF16),
            vm((128, 8, 1024), BF16),
            vm((128, 8, 1024), BF16),
            vm((128, 8, 1024), BF16),
            vm((128, 8, 1024), BF16),
            vm((512, 1024), F32),
            vm((2, TOK, 128), F32),
            dma((9,)),
            dma((3,)),
            dma((3,)),
            dma((7,)),
            dma((2,)),
            dma,
            dma,
            dma,
            dma,
            dma,
            dma,
            dma,
            dma((4,)),
            dma,
            dma((4,)),
            pltpu.SemaphoreType.REGULAR,
        ],
        compiler_params=pltpu.CompilerParams(
            collective_id=0, has_side_effects=True, vmem_limit_bytes=62 * 2**20
        ),
        name="layer",
    )(
        queries[0],
        keys[0],
        values[0],
        resid[0],
        out_weight,
        expert_gate[0],
        expert_up[0],
        expert_down[0],
        forget_cache[0],
        jnp.tile(query_gain, 2).reshape(1, 128),
        jnp.tile(key_gain, 2).reshape(1, 128),
        norm_gain.reshape(1, D),
        routes[0],
        group_weight,
        inner_share[0],
    )
    return out[None]


def solution(mesh):
    return jax.shard_map(
        shards,
        mesh=mesh,
        in_specs=(
            P("dp", "sp", None),
            P("dp", "sp", None),
            P("dp", "sp", None),
            P("dp", "sp", None),
            P("dp", "sp", None),
            P(),
            P(),
            P(None, "dp"),
            P(),
            P("dp", "sp", None),
            P("dp", "sp"),
            P("dp", "sp", None),
            P(("sp", "dp"), None, None),
            P(("sp", "dp"), None, None),
            P(("sp", "dp"), None, None),
        ),
        out_specs=P("dp", "sp", None),
        check_vma=False,
    )
```

```python
import functools

import jax
import jax.numpy as jnp
from jax import lax
from jax.experimental import pallas as pl
from jax.experimental.pallas import tpu as pltpu
from jax.sharding import PartitionSpec as P

EPS = 1e-06
MESH = pl.DeviceIdType.MESH
F32 = jnp.float32
BF16 = jnp.bfloat16
D = 2048
HD = 64
FF = 1024
TOK = 128
SEQ = 2048
QB = 256
MULT = 37
SP_MULT = 7


def dot(a, b):
    return jnp.dot(a, b, preferred_element_type=F32)


def drain(ref, sem):
    pltpu.make_async_copy(ref, ref, sem).wait()


def iota(shape, dim):
    return lax.broadcasted_iota(jnp.int32, shape, dim)


def mod(a, n):
    return lax.rem(a, n)


def kernel(
    q_h,
    k_h,
    v_h,
    resid_h,
    ow_h,
    eg_h,
    eu_h,
    ed_h,
    fc_ref,
    qg_ref,
    kg_ref,
    ng_ref,
    routes_ref,
    gw_ref,
    ish_ref,
    out_ref,
    qkv_s,
    qkv_r,
    qh,
    kt,
    ao,
    ar,
    probs,
    scale,
    wr,
    psend,
    precv,
    resid_s,
    disp,
    pick,
    perm,
    wg,
    wu,
    wd,
    send,
    recv,
    ysend,
    ret,
    acc,
    wts,
    loc_sem,
    qkv_send,
    qkv_recv,
    w_send,
    w_near,
    w_far,
    w_part,
    w_swap,
    a_send,
    a_recv,
    p_send,
    p_recv,
    d_send,
    d_recv,
    r_send,
    r_recv,
    ready,
):
    sp = lax.axis_index("sp")
    dp = lax.axis_index("dp")
    z, x = sp // 4, mod(sp, 4)
    y, c = dp // 2, mod(dp, 2)
    sign = 1 - 2 * c
    parity = mod(z + x, 2)

    local = []
    for n, (src, dst) in enumerate(
        (
            (k_h, qkv_s.at[0]),
            (q_h, qkv_s.at[1]),
            (v_h, qkv_s.at[2]),
            (ow_h.at[pl.ds(pl.multiple_of(c * 1024, 1024), 1024)],
             wr.at[:, pl.ds(pl.multiple_of(dp * 256, 256), 256)]),
            (resid_h, resid_s),
        )
    ):
        copy = pltpu.make_async_copy(src, dst, loc_sem.at[n])
        copy.start()
        local.append(copy)
    barrier = pltpu.get_barrier_semaphore()
    for k in range(1, 16):
        pl.semaphore_signal(barrier, inc=1, device_id=(mod(sp + k, 16), dp), device_id_type=MESH)
    for k in range(1, 8):
        pl.semaphore_signal(barrier, inc=1, device_id=(sp, mod(dp + k, 8)), device_id_type=MESH)
    pl.semaphore_wait(barrier, 22)

    def remote(src, dst, ssem, rsem, dev):
        return pltpu.make_async_remote_copy(
            src_ref=src, dst_ref=dst, send_sem=ssem, recv_sem=rsem, device_id=dev, device_id_type=MESH
        )

    my_cols = pl.ds(pl.multiple_of(dp * 256, 256), 256)

    def send_near(part, ssem, rsem):
        for step in (1, 3):
            for h in range(2):
                remote(
                    ow_h.at[pl.ds(pl.multiple_of(1024 * h + 512 * part, 512), 512)],
                    wr.at[pl.ds(pl.multiple_of(512 * part, 512), 512), my_cols],
                    ssem,
                    rsem,
                    (sp, mod(y + step, 4) * 2 + h),
                ).start()

    my_rows = pl.ds(pl.multiple_of(sp * TOK, TOK), TOK)
    for ten in range(3):
        local[ten].wait()

        def send_qkv(i, _, ten=ten):
            d = mod(SP_MULT * i, 16)
            t = mod(z + sign * (d // 4) + 4, 4) * 4 + mod(x + sign * mod(d, 4) + 4, 4)
            remote(
                qkv_s.at[ten, :, pl.ds(pl.multiple_of(t * 128, 128), 128)],
                qkv_r.at[ten, my_rows, :],
                qkv_send.at[ten],
                qkv_recv.at[ten],
                (t, dp),
            ).start()
            return 0

        lax.fori_loop(1, 16, send_qkv, 0)
        if ten == 0:
            send_near(parity, w_send.at[0], w_near.at[0])
            remote(
                ow_h.at[pl.ds(pl.multiple_of((1 - c) * 1024, 1024), 1024)],
                wr.at[:, my_cols],
                w_send.at[1],
                w_part,
                (sp, y * 2 + 1 - c),
            ).start()
        qkv_r[ten, my_rows, :] = qkv_s[ten, :, pl.ds(pl.multiple_of(sp * 128, 128), 128)]
    for k in range(1, 8):
        pl.semaphore_signal(ready, inc=1, device_id=(sp, mod(dp + k, 8)), device_id_type=MESH)
    experts = []
    for n, (src, dst) in enumerate(((eg_h, wg), (eu_h, wu), (ed_h, wd))):
        copy = pltpu.make_async_copy(src, dst, loc_sem.at[5 + n])
        copy.start()
        experts.append(copy)

    def expert_of(i):
        d = (MULT * i) & 127
        dz, dx, dy, dc = d & 3, (d >> 2) & 3, (d >> 4) & 3, d >> 6
        ts = ((z + sign * dz + 4) & 3) * 4 + ((x + sign * dx + 4) & 3)
        td = ((y + sign * dy + 4) & 3) * 2 + ((c + dc) & 1)
        return ts * 8 + td

    r_row = [
        jnp.broadcast_to(routes_ref[k : k + 1, :].astype(F32), (128, TOK)) for k in range(2)
    ]
    r_col = [m.T for m in r_row]
    lane = iota((TOK, 128), 1)
    sub = iota((TOK, 128), 0)
    hit_c = [(m == lane.astype(F32)).astype(F32) for m in r_col]
    hit_r = [(m == sub.astype(F32)).astype(F32) for m in r_row]
    lower = (lane < sub).astype(F32).astype(BF16)
    upper = (sub < lane).astype(F32).astype(BF16)
    before_c = dot(lower, (hit_c[0] + hit_c[1]).astype(BF16))
    before_r = dot((hit_r[0] + hit_r[1]).astype(BF16), upper)
    slot_c = [
        4.0 * r_col[k][:, :1] + jnp.sum(before_c * hit_c[k], axis=1, keepdims=True) for k in range(2)
    ]
    slot_r = [
        4.0 * r_row[k][:1, :] + jnp.sum(before_r * hit_r[k], axis=0, keepdims=True) for k in range(2)
    ]
    row = iota((1024, 128), 0)
    row_slot = (4 * expert_of(row >> 3) + (row & 3)).astype(F32)
    row_half = (row >> 2) & 1
    chosen = (row_slot == slot_r[0]) | (row_slot == slot_r[1])
    for g in range(2):
        disp[:, g * 128 : (g + 1) * 128] = jnp.where(chosen & (row_half == g), 1.0, 0.0).astype(BF16)
    col = iota((TOK, 1024), 1)
    col_slot = (4 * expert_of(col >> 3) + (col & 3)).astype(F32)
    col_half = (col >> 2) & 1
    for k in range(2):
        for g in range(2):
            at = (2 * k + g) * 128
            pick[at : at + 128, :] = jnp.where(
                (col_slot == slot_c[k]) & (col_half == g), 1.0, 0.0
            ).astype(BF16)
    share_sum = ish_ref[0:1, :] + ish_ref[1:2, :]
    for k in range(2):
        weight = gw_ref[...] * ish_ref[k : k + 1, :] / share_sum
        wts[k] = jnp.broadcast_to(weight, (128, TOK)).T
    p_o, p_i = iota((256, 256), 0), iota((256, 256), 1)
    perm[0] = jnp.where(
        p_i == 8 * ((p_o >> 2) & 31) + 4 * (p_o >> 7) + (p_o & 3), 1.0, 0.0
    ).astype(BF16)
    perm[1] = jnp.where(
        p_o == 8 * ((p_i >> 2) & 31) + 4 * (p_i >> 7) + (p_i & 3), 1.0, 0.0
    ).astype(BF16)

    def normed_heads(ten, at, size, gain_ref):
        rows = qkv_r[ten, at : at + size, :].astype(F32)
        square = rows * rows
        first = iota((size, 128), 1) < HD
        sum0 = jnp.sum(jnp.where(first, square, 0.0), axis=1, keepdims=True)
        sum1 = jnp.sum(jnp.where(first, 0.0, square), axis=1, keepdims=True)
        factor = jnp.where(
            first, lax.rsqrt(sum0 * (1.0 / HD) + EPS), lax.rsqrt(sum1 * (1.0 / HD) + EPS)
        )
        gain = jnp.concatenate([gain_ref[...]] * 2, axis=1)
        return (rows * factor * gain).astype(BF16).astype(F32)

    drain(qkv_r.at[0, pl.ds(0, 15 * TOK)], qkv_recv.at[0])
    step = 512
    for at in range(0, SEQ, step):
        turned = normed_heads(0, at, step, kg_ref).T
        sub = iota((128, step), 0)
        for h in range(2):
            bias = fc_ref[h : h + 1, at : at + step]
            high = bias.astype(BF16).astype(F32)
            middle = (bias - high).astype(BF16).astype(F32)
            low = bias - high - middle
            base = 64 * (1 - h)
            extra = jnp.where(
                sub == base, high, jnp.where(sub == base + 1, middle, jnp.where(sub == base + 2, low, 0.0))
            )
            mine = (sub < HD) if h == 0 else (sub >= HD)
            kt[h, :, at : at + step] = jnp.where(mine, turned, extra).astype(BF16)
    drain(qkv_r.at[1, pl.ds(0, 15 * TOK)], qkv_recv.at[1])
    for at in range(0, SEQ, step):
        scaled = normed_heads(1, at, step, qg_ref) * (HD**-0.5)
        lane = iota((step, 128), 1)
        for h in range(2):
            base = 64 * (1 - h)
            mine = (lane < HD) if h == 0 else (lane >= HD)
            extra = jnp.where((lane >= base) & (lane < base + 3), -1.0, 0.0)
            qh[h, at : at + step, :] = jnp.where(mine, scaled, extra).astype(BF16)

    drain(wr.at[pl.ds(0, 512), pl.ds(0, 1024)], w_near.at[0])
    for s, (near, onward) in enumerate(((3, 1), (1, 3))):
        part = wr.at[
            pl.ds(pl.multiple_of(512 * parity + 256 * s, 256), 256),
            pl.ds(pl.multiple_of(mod(y + near, 4) * 512, 512), 512),
        ]
        remote(part, part, w_send.at[2], w_far, (sp, mod(y + onward, 4) * 2 + c)).start()
    send_near(1 - parity, w_send.at[4], w_near.at[1])

    half = sp // 8
    a_cols = pl.ds(pl.multiple_of(mod(sp, 8) * 128, 128), 128)
    a_rows = pl.ds(pl.multiple_of(c * TOK, TOK), TOK)

    def return_block(i):
        for t in (2 * i, 2 * i + 1):
            own = jnp.logical_and(sp == t, half == c)
            rows = pl.ds(pl.multiple_of(t * TOK, TOK), TOK)

            @pl.when(own)
            def _(rows=rows):
                ar[a_rows, a_cols] = ao[rows, :]

            @pl.when(jnp.logical_not(own))
            def _(rows=rows, t=t):
                remote(ao.at[rows], ar.at[a_rows, a_cols], a_send, a_recv, (t, y * 2 + half)).start()

    blocks = SEQ // QB
    tri = iota((QB, QB), 1) <= iota((QB, QB), 0)
    first = iota((QB, 128), 1) < HD

    def weigh(i):
        at, keys = i * QB, (i + 1) * QB
        inverse = []
        for h in range(2):
            query = qh[h, at:keys, :]
            diag = jnp.where(tri, dot(query, kt[h, :, at:keys]), -jnp.inf)
            highest = jnp.max(diag, axis=1, keepdims=True)
            if at:
                past = dot(query, kt[h, :, :at])
                highest = jnp.maximum(highest, jnp.max(past, axis=1, keepdims=True))
            diag = jnp.exp(diag - highest)
            total = jnp.sum(diag, axis=1, keepdims=True)
            tile = i * (i + 1) // 2
            probs[h, tile + i] = diag.astype(BF16)
            if at:
                past = jnp.exp(past - highest)
                total = total + jnp.sum(past, axis=1, keepdims=True)
                for j in range(i):
                    probs[h, tile + j] = past[:, j * QB : (j + 1) * QB].astype(BF16)
            inverse.append(1.0 / total)
        scale[at:keys, :] = jnp.where(first, inverse[0], inverse[1])

    def combine(i):
        at, keys = i * QB, (i + 1) * QB
        results = []
        for h in range(2):
            result = None
            for j in range(i + 1):
                term = dot(probs[h, i * (i + 1) // 2 + j], qkv_r[2, j * QB : (j + 1) * QB, :])
                result = term if result is None else result + term
            results.append(result)
        ao[at:keys, :] = (jnp.where(first, results[0], results[1]) * scale[at:keys, :]).astype(BF16)

    def block_of(n):
        m = mod(n + sp // 2, blocks)
        odd = mod(m, 2)
        return (1 - odd) * (blocks - 1 - m // 2) + odd * (m // 2)

    for i in range(blocks):
        weigh(i)
    drain(qkv_r.at[2, pl.ds(0, 15 * TOK)], qkv_recv.at[2])

    def one_block(n, _):
        for i in range(blocks):
            pl.when(block_of(n) == i)(functools.partial(combine, i))
        return_block(block_of(n))
        return 0

    lax.fori_loop(0, blocks, one_block, 0)
    drain(wr.at[pl.ds(0, 512), pl.ds(0, 512)], w_far)
    for q, t in enumerate((
        z * 4 + mod(x + 1, 4), z * 4 + mod(x + 3, 4), mod(z + 1, 4) * 4 + x, mod(z + 3, 4) * 4 + x
    )):
        part = wr.at[
            pl.ds(pl.multiple_of(512 * parity + 128 * q, 128), 128),
            pl.ds(pl.multiple_of(mod(y + 2, 4) * 512, 512), 512),
        ]
        remote(part, part, w_send.at[3], w_swap, (t, dp)).start()

    local[3].wait()
    local[4].wait()
    drain(wr.at[:, pl.ds(0, 256)], w_part)
    drain(wr.at[pl.ds(0, 512), pl.ds(0, 1024)], w_near.at[1])
    drain(wr.at[pl.ds(0, 512), pl.ds(0, 512)], w_swap)
    own_in = half == c

    @pl.when(own_in)
    def _():
        drain(ao.at[pl.ds(0, 15 * TOK)], a_recv)
        drain(ao.at[pl.ds(0, 15 * TOK)], a_send)

    @pl.when(jnp.logical_not(own_in))
    def _():
        drain(ao.at[pl.ds(0, 16 * TOK)], a_recv)
        drain(ao.at[pl.ds(0, 16 * TOK)], a_send)

    other = ar[pl.ds(pl.multiple_of((1 - c) * TOK, TOK), TOK), :]
    for n in range(4):
        cols = pl.ds(512 * n, 512)
        psend[n] = dot(other, wr[:, cols])
        remote(psend.at[n], precv.at[n], p_send, p_recv, (sp, y * 2 + 1 - c)).start()
    mine = ar[a_rows, :]
    parts = [dot(mine, wr[:, 512 * n : 512 * n + 512]) for n in range(4)]
    drain(precv, p_recv)
    mids = []
    square = None
    for n in range(4):
        cols = slice(512 * n, 512 * n + 512)
        mid = (resid_s[:, cols].astype(F32) + (parts[n] + precv[n])).astype(BF16)
        resid_s[:, cols] = mid
        mid = mid.astype(F32)
        mids.append(mid)
        term = jnp.sum(mid * mid, axis=1, keepdims=True)
        square = term if square is None else square + term
    factor = lax.rsqrt(square * (1.0 / D) + EPS)
    normed = [
        (mids[n] * factor * ng_ref[:, 512 * n : 512 * n + 512]).astype(BF16) for n in range(4)
    ]
    halves = [jnp.concatenate(normed[2 * g : 2 * g + 2], axis=1) for g in range(2)]
    stacked = jnp.concatenate(halves, axis=0)
    for b in range(4):
        send[b * 32 : (b + 1) * 32] = (
            dot(disp[b * 256 : (b + 1) * 256, :], stacked).astype(BF16).reshape(32, 8, 1024)
        )

    pl.semaphore_wait(ready, 7)

    def partner(i, way):
        d = mod(MULT * i, 128)
        dz, dx, dy, dc = mod(d, 4), mod(d // 4, 4), mod(d // 16, 4), d // 64
        ts = mod(z + way * dz + 4, 4) * 4 + mod(x + way * dx + 4, 4)
        td = mod(y + way * dy + 4, 4) * 2 + mod(c + dc, 2)
        return ts, td

    def send_rows(i, _):
        remote(send.at[i], recv.at[i], d_send, d_recv.at[i // 32], partner(i, sign)).start()
        return 0

    lax.fori_loop(1, 128, send_rows, 0)
    recv[0] = send[0]
    for copy in experts:
        copy.wait()

    def wait_block(ref, sem, b):
        @pl.when(b == 0)
        def _():
            drain(ref.at[pl.ds(0, 31)], sem.at[b])

        @pl.when(b > 0)
        def _():
            drain(ref.at[pl.ds(0, 32)], sem.at[b])

    def run_expert(b, _):
        wait_block(recv, d_recv, b)
        at = pl.multiple_of(b * 32, 32)
        rows = recv[pl.ds(at, 32)].reshape(256, 1024)
        rows = dot(perm[0], rows).astype(BF16)
        gate = dot(rows[:128], wg[:1024, :]) + dot(rows[128:], wg[1024:, :])
        up = dot(rows[:128], wu[:1024, :]) + dot(rows[128:], wu[1024:, :])
        hidden = (gate / (1.0 + jnp.exp(-gate)) * up).astype(BF16)
        result = [dot(hidden, wd[:, g * 1024 : (g + 1) * 1024]).astype(BF16) for g in range(2)]
        back = dot(perm[1], jnp.concatenate(result, axis=0)).astype(BF16)
        ysend[pl.ds(at, 32)] = back.reshape(32, 8, 1024)

        def send_back(i, _):
            d = mod(MULT * i, 128)
            src_sign = sign * (1 - 2 * (d // 64))
            remote(ysend.at[i], ret.at[i], r_send, r_recv.at[b], partner(i, -src_sign)).start()
            return 0

        lax.fori_loop(jnp.where(b == 0, 1, b * 32), b * 32 + 32, send_back, 0)

        @pl.when(b == 0)
        def _():
            ret[0] = ysend[0]

        return 0

    lax.fori_loop(0, 4, run_expert, 0)
    acc[...] = jnp.zeros_like(acc)

    def collect(b, _):
        wait_block(ret, r_recv, b)
        rows = ret[pl.ds(pl.multiple_of(b * 32, 32), 32)].reshape(256, 1024)
        acc[...] += dot(pick[:, pl.ds(pl.multiple_of(b * 256, 256), 256)], rows)
        return 0

    lax.fori_loop(0, 4, collect, 0)
    for g in range(2):
        cols = slice(1024 * g, 1024 * g + 1024)
        mixed = wts[0][:, :1] * acc[g * 128 : g * 128 + 128, :]
        mixed = mixed + wts[1][:, :1] * acc[(2 + g) * 128 : (3 + g) * 128, :]
        out_ref[:, cols] = (resid_s[:, cols].astype(F32) + mixed).astype(BF16)

    for ten in range(3):
        drain(qkv_r.at[ten, pl.ds(0, 15 * TOK)], qkv_send.at[ten])
    drain(wr.at[pl.ds(0, 512), pl.ds(0, 1024)], w_send.at[0])
    drain(wr.at[:, pl.ds(0, 256)], w_send.at[1])
    drain(wr.at[pl.ds(0, 512), pl.ds(0, 512)], w_send.at[2])
    drain(wr.at[pl.ds(0, 512), pl.ds(0, 512)], w_send.at[3])
    drain(wr.at[pl.ds(0, 512), pl.ds(0, 1024)], w_send.at[4])
    drain(precv, p_send)
    drain(recv.at[pl.ds(0, 127)], d_send)
    drain(recv.at[pl.ds(0, 127)], r_send)


def shards(
    resid,
    queries,
    keys,
    values,
    forget_cache,
    query_gain,
    key_gain,
    out_weight,
    norm_gain,
    routes,
    group_weight,
    inner_share,
    expert_gate,
    expert_up,
    expert_down,
):
    hbm_spec = pl.BlockSpec(memory_space=pltpu.HBM)
    vmem_spec = pl.BlockSpec(memory_space=pltpu.VMEM)
    vm = pltpu.VMEM
    dma = pltpu.SemaphoreType.DMA
    out = pl.pallas_call(
        kernel,
        out_shape=jax.ShapeDtypeStruct((TOK, D), BF16),
        in_specs=[hbm_spec] * 8 + [vmem_spec] * 7,
        out_specs=vmem_spec,
        scratch_shapes=[
            vm((3, TOK, D), BF16),
            vm((3, SEQ, 128), BF16),
            vm((2, SEQ, 128), BF16),
            vm((2, 128, SEQ), BF16),
            vm((SEQ, 128), BF16),
            vm((2 * TOK, 1024), BF16),
            vm((2, 36, QB, QB), BF16),
            vm((SEQ, 128), F32),
            vm((1024, D), BF16),
            vm((4, TOK, 512), F32),
            vm((4, TOK, 512), F32),
            vm((TOK, D), BF16),
            vm((1024, 256), BF16),
            vm((512, 1024), BF16),
            vm((2, 256, 256), BF16),
            vm((D, FF), BF16),
            vm((D, FF), BF16),
            vm((FF, D), BF16),
            vm((128, 8, 1024), BF16),
            vm((128, 8, 1024), BF16),
            vm((128, 8, 1024), BF16),
            vm((128, 8, 1024), BF16),
            vm((512, 1024), F32),
            vm((2, TOK, 128), F32),
            dma((9,)),
            dma((3,)),
            dma((3,)),
            dma((5,)),
            dma((2,)),
            dma,
            dma,
            dma,
            dma,
            dma,
            dma,
            dma,
            dma,
            dma((4,)),
            dma,
            dma((4,)),
            pltpu.SemaphoreType.REGULAR,
        ],
        compiler_params=pltpu.CompilerParams(
            collective_id=0, has_side_effects=True, vmem_limit_bytes=53 * 2**20
        ),
        name="layer",
    )(
        *[
            pltpu.with_memory_space_constraint(a, pltpu.HBM)
            for a in (
                queries[0],
                keys[0],
                values[0],
                resid[0],
                out_weight,
                expert_gate[0],
                expert_up[0],
                expert_down[0],
                forget_cache[0],
                query_gain.reshape(1, HD),
                key_gain.reshape(1, HD),
                norm_gain.reshape(1, D),
                routes[0].T,
                group_weight,
                inner_share[0].T,
            )
        ]
    )
    return out[None]


def solution(mesh):
    return jax.shard_map(
        shards,
        mesh=mesh,
        in_specs=(
            P("dp", "sp", None),
            P("dp", "sp", None),
            P("dp", "sp", None),
            P("dp", "sp", None),
            P("dp", "sp", None),
            P(),
            P(),
            P(None, "dp"),
            P(),
            P("dp", "sp", None),
            P("dp", "sp"),
            P("dp", "sp", None),
            P(("sp", "dp"), None, None),
            P(("sp", "dp"), None, None),
            P(("sp", "dp"), None, None),
        ),
        out_specs=P("dp", "sp", None),
        check_vma=False,
    )
```

```python
import functools

import jax
import jax.numpy as jnp
from jax import lax
from jax.experimental import pallas as pl
from jax.experimental.pallas import tpu as pltpu
from jax.sharding import PartitionSpec as P

EPS = 1e-06
MESH = pl.DeviceIdType.MESH
F32 = jnp.float32
BF16 = jnp.bfloat16
D = 2048
HD = 64
FF = 1024
TOK = 128
SEQ = 2048
QB = 256
MULT = 27
SP_MULT = 7


def dot(a, b):
    return jnp.dot(a, b, preferred_element_type=F32)


def drain(ref, sem):
    pltpu.make_async_copy(ref, ref, sem).wait()


def iota(shape, dim):
    return lax.broadcasted_iota(jnp.int32, shape, dim)


def mod(a, n):
    return lax.rem(a, n)


def kernel(
    q_h,
    k_h,
    v_h,
    resid_h,
    ow_h,
    eg_h,
    eu_h,
    ed_h,
    fc_h,
    qg_h,
    kg_h,
    ng_h,
    routes_h,
    gw_h,
    ish_h,
    out_ref,
    fc_ref,
    qg_ref,
    kg_ref,
    ng_ref,
    routes_ref,
    gw_ref,
    ish_ref,
    qkv_s,
    qkv_r,
    qh,
    kt,
    ao,
    ar,
    probs,
    scale,
    wr,
    psend,
    precv,
    resid_s,
    disp,
    pick,
    perm,
    wg,
    wu,
    wd,
    send,
    recv,
    ysend,
    ret,
    acc,
    wts,
    loc_sem,
    qkv_send,
    qkv_recv,
    w_send,
    w_near,
    w_far,
    w_part,
    a_send,
    a_recv,
    p_send,
    p_recv,
    d_send,
    d_recv,
    r_send,
    r_recv,
    ready,
):
    sp = lax.axis_index("sp")
    dp = lax.axis_index("dp")
    z, x = sp // 4, mod(sp, 4)
    y, c = dp // 2, mod(dp, 2)
    sign = 1 - 2 * c
    parity = mod(z + x, 2)

    barrier = pltpu.get_barrier_semaphore()
    for k in range(1, 16):
        pl.semaphore_signal(barrier, inc=1, device_id=(mod(sp + k, 16), dp), device_id_type=MESH)
    for k in range(1, 8):
        pl.semaphore_signal(barrier, inc=1, device_id=(sp, mod(dp + k, 8)), device_id_type=MESH)
    local = []
    for n, (src, dst) in enumerate(
        (
            (k_h, qkv_s.at[0]),
            (q_h, qkv_s.at[1]),
            (v_h, qkv_s.at[2]),
            (ow_h.at[pl.ds(pl.multiple_of(c * 1024, 1024), 1024)],
             wr.at[:, pl.ds(pl.multiple_of(dp * 256, 256), 256)]),
            (resid_h, resid_s),
            (routes_h, routes_ref),
            (gw_h, gw_ref),
            (ish_h, ish_ref),
            (fc_h, fc_ref),
            (kg_h, kg_ref),
            (qg_h, qg_ref),
            (ng_h, ng_ref),
        )
    ):
        copy = pltpu.make_async_copy(src, dst, loc_sem.at[n])
        copy.start()
        local.append(copy)
    pl.semaphore_wait(barrier, 22)

    def remote(src, dst, ssem, rsem, dev):
        return pltpu.make_async_remote_copy(
            src_ref=src, dst_ref=dst, send_sem=ssem, recv_sem=rsem, device_id=dev, device_id_type=MESH
        )

    my_cols = pl.ds(pl.multiple_of(dp * 256, 256), 256)

    def send_near(start, size, ssem, rsem):
        for step in (1, 3):
            for h in range(2):
                remote(
                    ow_h.at[pl.ds(pl.multiple_of(1024 * h + start, 256), size)],
                    wr.at[pl.ds(pl.multiple_of(start, 256), size), my_cols],
                    ssem,
                    rsem,
                    (sp, mod(y + step, 4) * 2 + h),
                ).start()

    my_rows = pl.ds(pl.multiple_of(sp * TOK, TOK), TOK)
    for ten in range(3):
        local[ten].wait()

        def send_qkv(i, _, ten=ten):
            d = mod(SP_MULT * i, 16)
            t = mod(z + sign * (d // 4) + 4, 4) * 4 + mod(x + sign * mod(d, 4) + 4, 4)
            remote(
                qkv_s.at[ten, :, pl.ds(pl.multiple_of(t * 128, 128), 128)],
                qkv_r.at[ten, my_rows, :],
                qkv_send.at[ten],
                qkv_recv.at[ten],
                (t, dp),
            ).start()
            return 0

        lax.fori_loop(1, 16, send_qkv, 0)
        if ten == 0:
            send_near(512 * parity, 512, w_send.at[0], w_near.at[0])
            send_near(512 * (1 - parity), 256, w_send.at[4], w_near.at[1])
            remote(
                ow_h.at[pl.ds(pl.multiple_of((1 - c) * 1024, 1024), 1024)],
                wr.at[:, my_cols],
                w_send.at[1],
                w_part,
                (sp, y * 2 + 1 - c),
            ).start()
        qkv_r[ten, my_rows, :] = qkv_s[ten, :, pl.ds(pl.multiple_of(sp * 128, 128), 128)]
    for k in range(1, 8):
        pl.semaphore_signal(ready, inc=1, device_id=(sp, mod(dp + k, 8)), device_id_type=MESH)
    experts = []
    for n, (src, dst) in enumerate(((eg_h, wg), (eu_h, wu), (ed_h, wd))):
        copy = pltpu.make_async_copy(src, dst, loc_sem.at[12 + n])
        copy.start()
        experts.append(copy)

    for copy in local[5:]:
        copy.wait()

    def expert_of(i):
        d = (MULT * i) & 127
        dz, dx, dy, dc = d & 3, (d >> 2) & 3, (d >> 4) & 3, d >> 6
        ts = ((z + sign * dz + 4) & 3) * 4 + ((x + sign * dx + 4) & 3)
        td = ((y + sign * dy + 4) & 3) * 2 + ((c + dc) & 1)
        return ts * 8 + td

    r_row = [
        jnp.broadcast_to(routes_ref[k : k + 1, :].astype(F32), (128, TOK)) for k in range(2)
    ]
    r_col = [m.T for m in r_row]
    lane = iota((TOK, 128), 1)
    sub = iota((TOK, 128), 0)
    hit_c = [(m == lane.astype(F32)).astype(F32) for m in r_col]
    hit_r = [(m == sub.astype(F32)).astype(F32) for m in r_row]
    lower = (lane < sub).astype(F32).astype(BF16)
    upper = (sub < lane).astype(F32).astype(BF16)
    before_c = dot(lower, (hit_c[0] + hit_c[1]).astype(BF16))
    before_r = dot((hit_r[0] + hit_r[1]).astype(BF16), upper)
    slot_c = [
        4.0 * r_col[k][:, :1] + jnp.sum(before_c * hit_c[k], axis=1, keepdims=True) for k in range(2)
    ]
    slot_r = [
        4.0 * r_row[k][:1, :] + jnp.sum(before_r * hit_r[k], axis=0, keepdims=True) for k in range(2)
    ]
    row = iota((1024, 128), 0)
    row_slot = (4 * expert_of(row >> 3) + (row & 3)).astype(F32)
    row_half = (row >> 2) & 1
    chosen = (row_slot == slot_r[0]) | (row_slot == slot_r[1])
    for g in range(2):
        disp[:, g * 128 : (g + 1) * 128] = jnp.where(chosen & (row_half == g), 1.0, 0.0).astype(BF16)
    col = iota((TOK, 1024), 1)
    col_slot = (4 * expert_of(col >> 3) + (col & 3)).astype(F32)
    col_half = (col >> 2) & 1
    for k in range(2):
        for g in range(2):
            at = (2 * k + g) * 128
            pick[at : at + 128, :] = jnp.where(
                (col_slot == slot_c[k]) & (col_half == g), 1.0, 0.0
            ).astype(BF16)
    share_sum = ish_ref[0:1, :] + ish_ref[1:2, :]
    for k in range(2):
        weight = gw_ref[...] * ish_ref[k : k + 1, :] / share_sum
        wts[k] = jnp.broadcast_to(weight, (128, TOK)).T
    p_o, p_i = iota((256, 256), 0), iota((256, 256), 1)
    perm[0] = jnp.where(
        p_i == 8 * ((p_o >> 2) & 31) + 4 * (p_o >> 7) + (p_o & 3), 1.0, 0.0
    ).astype(BF16)
    perm[1] = jnp.where(
        p_o == 8 * ((p_i >> 2) & 31) + 4 * (p_i >> 7) + (p_i & 3), 1.0, 0.0
    ).astype(BF16)

    def normed_heads(ten, at, size, gain_ref):
        rows = qkv_r[ten, at : at + size, :].astype(F32)
        square = rows * rows
        first = iota((size, 128), 1) < HD
        sum0 = jnp.sum(jnp.where(first, square, 0.0), axis=1, keepdims=True)
        sum1 = jnp.sum(jnp.where(first, 0.0, square), axis=1, keepdims=True)
        factor = jnp.where(
            first, lax.rsqrt(sum0 * (1.0 / HD) + EPS), lax.rsqrt(sum1 * (1.0 / HD) + EPS)
        )
        gain = jnp.concatenate([gain_ref[...]] * 2, axis=1)
        return (rows * factor * gain).astype(BF16).astype(F32)

    drain(qkv_r.at[0, pl.ds(0, 15 * TOK)], qkv_recv.at[0])
    step = 512
    for at in range(0, SEQ, step):
        turned = normed_heads(0, at, step, kg_ref).T
        sub = iota((128, step), 0)
        for h in range(2):
            bias = fc_ref[h : h + 1, at : at + step]
            high = bias.astype(BF16).astype(F32)
            middle = (bias - high).astype(BF16).astype(F32)
            low = bias - high - middle
            base = 64 * (1 - h)
            extra = jnp.where(
                sub == base, high, jnp.where(sub == base + 1, middle, jnp.where(sub == base + 2, low, 0.0))
            )
            mine = (sub < HD) if h == 0 else (sub >= HD)
            kt[h, :, at : at + step] = jnp.where(mine, turned, extra).astype(BF16)
    drain(qkv_r.at[1, pl.ds(0, 15 * TOK)], qkv_recv.at[1])
    for at in range(0, SEQ, step):
        scaled = normed_heads(1, at, step, qg_ref) * (HD**-0.5)
        lane = iota((step, 128), 1)
        for h in range(2):
            base = 64 * (1 - h)
            mine = (lane < HD) if h == 0 else (lane >= HD)
            extra = jnp.where((lane >= base) & (lane < base + 3), -1.0, 0.0)
            qh[h, at : at + step, :] = jnp.where(mine, scaled, extra).astype(BF16)

    drain(wr.at[pl.ds(0, 512), pl.ds(0, 1024)], w_near.at[0])
    def relay(start, ssem, rsem):
        for s, (near, onward) in enumerate(((3, 1), (1, 3))):
            part = wr.at[
                pl.ds(pl.multiple_of(start + 256 * s, 256), 256),
                pl.ds(pl.multiple_of(mod(y + near, 4) * 512, 512), 512),
            ]
            remote(part, part, ssem, rsem, (sp, mod(y + onward, 4) * 2 + c)).start()

    relay(512 * parity, w_send.at[2], w_far.at[0])
    across = (
        z * 4 + mod(x + 1, 4), z * 4 + mod(x + 3, 4), mod(z + 1, 4) * 4 + x, mod(z + 3, 4) * 4 + x
    )

    for step in (1, 3):
        for q, t in enumerate(across):
            part = wr.at[
                pl.ds(pl.multiple_of(512 * parity + 256 + 64 * q, 64), 64),
                pl.ds(pl.multiple_of(mod(y + step, 4) * 512, 512), 512),
            ]
            remote(part, part, w_send.at[5], w_near.at[2], (t, dp)).start()

    half = sp // 8
    a_cols = pl.ds(pl.multiple_of(mod(sp, 8) * 128, 128), 128)
    a_rows = pl.ds(pl.multiple_of(c * TOK, TOK), TOK)

    def return_block(i):
        for t in (2 * i, 2 * i + 1):
            own = jnp.logical_and(sp == t, half == c)
            rows = pl.ds(pl.multiple_of(t * TOK, TOK), TOK)

            @pl.when(own)
            def _(rows=rows):
                ar[a_rows, a_cols] = ao[rows, :]

            @pl.when(jnp.logical_not(own))
            def _(rows=rows, t=t):
                remote(ao.at[rows], ar.at[a_rows, a_cols], a_send, a_recv, (t, y * 2 + half)).start()

    blocks = SEQ // QB
    tri = iota((QB, QB), 1) <= iota((QB, QB), 0)
    first = iota((QB, 128), 1) < HD

    def weigh(i):
        at, keys = i * QB, (i + 1) * QB
        inverse = []
        for h in range(2):
            query = qh[h, at:keys, :]
            diag = jnp.where(tri, dot(query, kt[h, :, at:keys]), -jnp.inf)
            highest = jnp.max(diag, axis=1, keepdims=True)
            if at:
                past = dot(query, kt[h, :, :at])
                highest = jnp.maximum(highest, jnp.max(past, axis=1, keepdims=True))
            diag = jnp.exp(diag - highest)
            total = jnp.sum(diag, axis=1, keepdims=True)
            tile = i * (i + 1) // 2
            probs[h, tile + i] = diag.astype(BF16)
            if at:
                past = jnp.exp(past - highest)
                total = total + jnp.sum(past, axis=1, keepdims=True)
                for j in range(i):
                    probs[h, tile + j] = past[:, j * QB : (j + 1) * QB].astype(BF16)
            inverse.append(1.0 / total)
        scale[at:keys, :] = jnp.where(first, inverse[0], inverse[1])

    def combine(i):
        at, keys = i * QB, (i + 1) * QB
        results = []
        for h in range(2):
            result = None
            for j in range(i + 1):
                term = dot(probs[h, i * (i + 1) // 2 + j], qkv_r[2, j * QB : (j + 1) * QB, :])
                result = term if result is None else result + term
            results.append(result)
        ao[at:keys, :] = (jnp.where(first, results[0], results[1]) * scale[at:keys, :]).astype(BF16)

    def block_of(n):
        m = mod(n + sp // 2, blocks)
        odd = mod(m, 2)
        return (1 - odd) * (blocks - 1 - m // 2) + odd * (m // 2)

    for i in range(blocks):
        weigh(i)
    drain(qkv_r.at[2, pl.ds(0, 15 * TOK)], qkv_recv.at[2])
    drain(wr.at[pl.ds(0, 256), pl.ds(0, 1024)], w_near.at[1])
    drain(wr.at[pl.ds(0, 256), pl.ds(0, 1024)], w_near.at[2])
    relay(512 * (1 - parity), w_send.at[3], w_far.at[1])

    def one_block(n, _):
        for i in range(blocks):
            pl.when(block_of(n) == i)(functools.partial(combine, i))
        return_block(block_of(n))
        return 0

    lax.fori_loop(0, blocks, one_block, 0)

    local[3].wait()
    local[4].wait()
    drain(wr.at[:, pl.ds(0, 256)], w_part)
    drain(wr.at[pl.ds(0, 512), pl.ds(0, 512)], w_far.at[0])
    drain(wr.at[pl.ds(0, 512), pl.ds(0, 512)], w_far.at[1])
    own_in = half == c

    @pl.when(own_in)
    def _():
        drain(ao.at[pl.ds(0, 15 * TOK)], a_recv)
        drain(ao.at[pl.ds(0, 15 * TOK)], a_send)

    @pl.when(jnp.logical_not(own_in))
    def _():
        drain(ao.at[pl.ds(0, 16 * TOK)], a_recv)
        drain(ao.at[pl.ds(0, 16 * TOK)], a_send)

    other = ar[pl.ds(pl.multiple_of((1 - c) * TOK, TOK), TOK), :]
    for n in range(4):
        cols = pl.ds(512 * n, 512)
        psend[n] = dot(other, wr[:, cols])
        remote(psend.at[n], precv.at[n], p_send, p_recv, (sp, y * 2 + 1 - c)).start()
    mine = ar[a_rows, :]
    parts = [dot(mine, wr[:, 512 * n : 512 * n + 512]) for n in range(4)]
    drain(precv, p_recv)
    mids = []
    square = None
    for n in range(4):
        cols = slice(512 * n, 512 * n + 512)
        mid = (resid_s[:, cols].astype(F32) + (parts[n] + precv[n])).astype(BF16)
        resid_s[:, cols] = mid
        mid = mid.astype(F32)
        mids.append(mid)
        term = jnp.sum(mid * mid, axis=1, keepdims=True)
        square = term if square is None else square + term
    factor = lax.rsqrt(square * (1.0 / D) + EPS)
    normed = [
        (mids[n] * factor * ng_ref[:, 512 * n : 512 * n + 512]).astype(BF16) for n in range(4)
    ]
    halves = [jnp.concatenate(normed[2 * g : 2 * g + 2], axis=1) for g in range(2)]
    stacked = jnp.concatenate(halves, axis=0)
    pl.semaphore_wait(ready, 7)

    def partner(i, way):
        d = mod(MULT * i, 128)
        dz, dx, dy, dc = mod(d, 4), mod(d // 4, 4), mod(d // 16, 4), d // 64
        ts = mod(z + way * dz + 4, 4) * 4 + mod(x + way * dx + 4, 4)
        td = mod(y + way * dy + 4, 4) * 2 + mod(c + dc, 2)
        return ts, td

    def send_rows(i, _):
        remote(send.at[i], recv.at[i], d_send, d_recv.at[i // 32], partner(i, sign)).start()
        return 0

    for b in range(4):
        send[b * 32 : (b + 1) * 32] = (
            dot(disp[b * 256 : (b + 1) * 256, :], stacked).astype(BF16).reshape(32, 8, 1024)
        )
        lax.fori_loop(max(1, b * 32), b * 32 + 32, send_rows, 0)
    recv[0] = send[0]
    for copy in experts:
        copy.wait()

    def wait_block(ref, sem, b):
        @pl.when(b == 0)
        def _():
            drain(ref.at[pl.ds(0, 31)], sem.at[b])

        @pl.when(b > 0)
        def _():
            drain(ref.at[pl.ds(0, 32)], sem.at[b])

    def run_expert(b, _):
        wait_block(recv, d_recv, b)
        at = pl.multiple_of(b * 32, 32)
        rows = recv[pl.ds(at, 32)].reshape(256, 1024)
        rows = dot(perm[0], rows).astype(BF16)
        gate = dot(rows[:128], wg[:1024, :]) + dot(rows[128:], wg[1024:, :])
        up = dot(rows[:128], wu[:1024, :]) + dot(rows[128:], wu[1024:, :])
        hidden = (gate / (1.0 + jnp.exp(-gate)) * up).astype(BF16)
        result = [dot(hidden, wd[:, g * 1024 : (g + 1) * 1024]).astype(BF16) for g in range(2)]
        back = dot(perm[1], jnp.concatenate(result, axis=0)).astype(BF16)
        ysend[pl.ds(at, 32)] = back.reshape(32, 8, 1024)

        def send_back(i, _):
            d = mod(MULT * i, 128)
            src_sign = sign * (1 - 2 * (d // 64))
            remote(ysend.at[i], ret.at[i], r_send, r_recv.at[b], partner(i, -src_sign)).start()
            return 0

        lax.fori_loop(jnp.where(b == 0, 1, b * 32), b * 32 + 32, send_back, 0)

        @pl.when(b == 0)
        def _():
            ret[0] = ysend[0]

        return 0

    lax.fori_loop(0, 4, run_expert, 0)
    acc[...] = jnp.zeros_like(acc)

    def collect(b, _):
        wait_block(ret, r_recv, b)
        rows = ret[pl.ds(pl.multiple_of(b * 32, 32), 32)].reshape(256, 1024)
        acc[...] += dot(pick[:, pl.ds(pl.multiple_of(b * 256, 256), 256)], rows)
        return 0

    lax.fori_loop(0, 4, collect, 0)
    for g in range(2):
        cols = slice(1024 * g, 1024 * g + 1024)
        mixed = wts[0][:, :1] * acc[g * 128 : g * 128 + 128, :]
        mixed = mixed + wts[1][:, :1] * acc[(2 + g) * 128 : (3 + g) * 128, :]
        out_ref[:, cols] = (resid_s[:, cols].astype(F32) + mixed).astype(BF16)

    for ten in range(3):
        drain(qkv_r.at[ten, pl.ds(0, 15 * TOK)], qkv_send.at[ten])
    drain(wr.at[pl.ds(0, 512), pl.ds(0, 1024)], w_send.at[0])
    drain(wr.at[:, pl.ds(0, 256)], w_send.at[1])
    drain(wr.at[pl.ds(0, 512), pl.ds(0, 512)], w_send.at[2])
    drain(wr.at[pl.ds(0, 512), pl.ds(0, 512)], w_send.at[3])
    drain(wr.at[pl.ds(0, 256), pl.ds(0, 1024)], w_send.at[4])
    drain(wr.at[pl.ds(0, 256), pl.ds(0, 1024)], w_send.at[5])
    drain(precv, p_send)
    drain(recv.at[pl.ds(0, 127)], d_send)
    drain(recv.at[pl.ds(0, 127)], r_send)


def shards(
    resid,
    queries,
    keys,
    values,
    forget_cache,
    query_gain,
    key_gain,
    out_weight,
    norm_gain,
    routes,
    group_weight,
    inner_share,
    expert_gate,
    expert_up,
    expert_down,
):
    hbm_spec = pl.BlockSpec(memory_space=pltpu.HBM)
    vmem_spec = pl.BlockSpec(memory_space=pltpu.VMEM)
    vm = pltpu.VMEM
    dma = pltpu.SemaphoreType.DMA
    out = pl.pallas_call(
        kernel,
        out_shape=jax.ShapeDtypeStruct((TOK, D), BF16),
        in_specs=[hbm_spec] * 15,
        out_specs=vmem_spec,
        scratch_shapes=[
            vm((2, SEQ), F32),
            vm((1, HD), F32),
            vm((1, HD), F32),
            vm((1, D), F32),
            vm((2, TOK), jnp.int32),
            vm((1, TOK), F32),
            vm((2, TOK), F32),
            vm((3, TOK, D), BF16),
            vm((3, SEQ, 128), BF16),
            vm((2, SEQ, 128), BF16),
            vm((2, 128, SEQ), BF16),
            vm((SEQ, 128), BF16),
            vm((2 * TOK, 1024), BF16),
            vm((2, 36, QB, QB), BF16),
            vm((SEQ, 128), F32),
            vm((1024, D), BF16),
            vm((4, TOK, 512), F32),
            vm((4, TOK, 512), F32),
            vm((TOK, D), BF16),
            vm((1024, 256), BF16),
            vm((512, 1024), BF16),
            vm((2, 256, 256), BF16),
            vm((D, FF), BF16),
            vm((D, FF), BF16),
            vm((FF, D), BF16),
            vm((128, 8, 1024), BF16),
            vm((128, 8, 1024), BF16),
            vm((128, 8, 1024), BF16),
            vm((128, 8, 1024), BF16),
            vm((512, 1024), F32),
            vm((2, TOK, 128), F32),
            dma((15,)),
            dma((3,)),
            dma((3,)),
            dma((6,)),
            dma((3,)),
            dma((2,)),
            dma,
            dma,
            dma,
            dma,
            dma,
            dma,
            dma((4,)),
            dma,
            dma((4,)),
            pltpu.SemaphoreType.REGULAR,
        ],
        compiler_params=pltpu.CompilerParams(
            collective_id=0, has_side_effects=True, vmem_limit_bytes=53 * 2**20
        ),
        name="layer",
    )(
        *[
            pltpu.with_memory_space_constraint(a, pltpu.HBM)
            for a in (
                queries[0],
                keys[0],
                values[0],
                resid[0],
                out_weight,
                expert_gate[0],
                expert_up[0],
                expert_down[0],
                forget_cache[0],
                query_gain.reshape(1, HD),
                key_gain.reshape(1, HD),
                norm_gain.reshape(1, D),
                routes[0].T,
                group_weight,
                inner_share[0].T,
            )
        ]
    )
    return out[None]


def solution(mesh):
    return jax.shard_map(
        shards,
        mesh=mesh,
        in_specs=(
            P("dp", "sp", None),
            P("dp", "sp", None),
            P("dp", "sp", None),
            P("dp", "sp", None),
            P("dp", "sp", None),
            P(),
            P(),
            P(None, "dp"),
            P(),
            P("dp", "sp", None),
            P("dp", "sp"),
            P("dp", "sp", None),
            P(("sp", "dp"), None, None),
            P(("sp", "dp"), None, None),
            P(("sp", "dp"), None, None),
        ),
        out_specs=P("dp", "sp", None),
        check_vma=False,
    )
```

```python
import functools

import jax
import jax.numpy as jnp
from jax import lax
from jax.experimental import pallas as pl
from jax.experimental.pallas import tpu as pltpu
from jax.sharding import PartitionSpec as P

EPS = 1e-06
MESH = pl.DeviceIdType.MESH
F32 = jnp.float32
BF16 = jnp.bfloat16
D = 2048
HD = 64
FF = 1024
TOK = 128
SEQ = 2048
QB = 256
MULT = 27
SP_MULT = 7


def dot(a, b):
    return jnp.dot(a, b, preferred_element_type=F32)


def drain(ref, sem):
    pltpu.make_async_copy(ref, ref, sem).wait()


def iota(shape, dim):
    return lax.broadcasted_iota(jnp.int32, shape, dim)


def mod(a, n):
    return lax.rem(a, n)


def kernel(
    q_h,
    k_h,
    v_h,
    resid_h,
    ow_h,
    eg_h,
    eu_h,
    ed_h,
    fc_h,
    qg_h,
    kg_h,
    ng_h,
    routes_h,
    gw_h,
    ish_h,
    out_ref,
    fc_ref,
    qg_ref,
    kg_ref,
    ng_ref,
    routes_ref,
    gw_ref,
    ish_ref,
    qkv_s,
    qkv_r,
    qh,
    kt,
    ao,
    ar,
    probs,
    scale,
    wr,
    psend,
    precv,
    resid_s,
    disp,
    pick,
    perm,
    wg,
    wu,
    wd,
    send,
    recv,
    ysend,
    ret,
    acc,
    wts,
    loc_sem,
    qkv_send,
    qkv_recv,
    w_send,
    w_near,
    w_far,
    w_part,
    a_send,
    a_recv,
    p_send,
    p_recv,
    d_send,
    d_recv,
    r_send,
    r_recv,
    ready,
):
    sp = lax.axis_index("sp")
    dp = lax.axis_index("dp")
    z, x = sp // 4, mod(sp, 4)
    y, c = dp // 2, mod(dp, 2)
    sign = 1 - 2 * c
    parity = mod(z + x, 2)

    barrier = pltpu.get_barrier_semaphore()
    for k in range(1, 16):
        pl.semaphore_signal(barrier, inc=1, device_id=(mod(sp + k, 16), dp), device_id_type=MESH)
    for k in range(1, 8):
        pl.semaphore_signal(barrier, inc=1, device_id=(sp, mod(dp + k, 8)), device_id_type=MESH)
    local = []
    for n, (src, dst) in enumerate(
        (
            (k_h, qkv_s.at[0]),
            (q_h, qkv_s.at[1]),
            (v_h, qkv_s.at[2]),
            (ow_h.at[pl.ds(pl.multiple_of(c * 1024, 1024), 1024)],
             wr.at[:, pl.ds(pl.multiple_of(dp * 256, 256), 256)]),
            (resid_h, resid_s),
            (routes_h, routes_ref),
            (gw_h, gw_ref),
            (ish_h, ish_ref),
            (fc_h, fc_ref),
            (kg_h, kg_ref),
            (qg_h, qg_ref),
            (ng_h, ng_ref),
        )
    ):
        copy = pltpu.make_async_copy(src, dst, loc_sem.at[n])
        copy.start()
        local.append(copy)
    pl.semaphore_wait(barrier, 22)

    def remote(src, dst, ssem, rsem, dev):
        return pltpu.make_async_remote_copy(
            src_ref=src, dst_ref=dst, send_sem=ssem, recv_sem=rsem, device_id=dev, device_id_type=MESH
        )

    my_cols = pl.ds(pl.multiple_of(dp * 256, 256), 256)

    def send_near(start, size, ssem, rsem):
        for step in (1, 3):
            for h in range(2):
                remote(
                    ow_h.at[pl.ds(pl.multiple_of(1024 * h + start, 256), size)],
                    wr.at[pl.ds(pl.multiple_of(start, 256), size), my_cols],
                    ssem,
                    rsem,
                    (sp, mod(y + step, 4) * 2 + h),
                ).start()

    my_rows = pl.ds(pl.multiple_of(sp * TOK, TOK), TOK)
    for ten in range(3):
        local[ten].wait()

        def send_qkv(i, _, ten=ten):
            d = mod(SP_MULT * i, 16)
            t = mod(z + sign * (d // 4) + 4, 4) * 4 + mod(x + sign * mod(d, 4) + 4, 4)
            remote(
                qkv_s.at[ten, :, pl.ds(pl.multiple_of(t * 128, 128), 128)],
                qkv_r.at[ten, my_rows, :],
                qkv_send.at[ten],
                qkv_recv.at[ten],
                (t, dp),
            ).start()
            return 0

        lax.fori_loop(1, 16, send_qkv, 0)
        if ten == 0:
            send_near(512 * parity, 512, w_send.at[0], w_near.at[0])
            send_near(512 * (1 - parity), 256, w_send.at[4], w_near.at[1])
            remote(
                ow_h.at[pl.ds(pl.multiple_of((1 - c) * 1024, 1024), 1024)],
                wr.at[:, my_cols],
                w_send.at[1],
                w_part,
                (sp, y * 2 + 1 - c),
            ).start()
        qkv_r[ten, my_rows, :] = qkv_s[ten, :, pl.ds(pl.multiple_of(sp * 128, 128), 128)]
    for k in range(1, 8):
        pl.semaphore_signal(ready, inc=1, device_id=(sp, mod(dp + k, 8)), device_id_type=MESH)
    experts = []
    for n, (src, dst) in enumerate(((eg_h, wg), (eu_h, wu), (ed_h, wd))):
        copy = pltpu.make_async_copy(src, dst, loc_sem.at[12 + n])
        copy.start()
        experts.append(copy)

    for copy in local[5:]:
        copy.wait()

    def expert_of(i):
        d = (MULT * i) & 127
        dz, dx, dy, dc = d & 3, (d >> 2) & 3, (d >> 4) & 3, d >> 6
        ts = ((z + sign * dz + 4) & 3) * 4 + ((x + sign * dx + 4) & 3)
        td = ((y + sign * dy + 4) & 3) * 2 + ((c + dc) & 1)
        return ts * 8 + td

    r_row = [
        jnp.broadcast_to(routes_ref[k : k + 1, :].astype(F32), (128, TOK)) for k in range(2)
    ]
    r_col = [m.T for m in r_row]
    lane = iota((TOK, 128), 1)
    sub = iota((TOK, 128), 0)
    hit_c = [(m == lane.astype(F32)).astype(F32) for m in r_col]
    hit_r = [(m == sub.astype(F32)).astype(F32) for m in r_row]
    lower = (lane < sub).astype(F32).astype(BF16)
    upper = (sub < lane).astype(F32).astype(BF16)
    before_c = dot(lower, (hit_c[0] + hit_c[1]).astype(BF16))
    before_r = dot((hit_r[0] + hit_r[1]).astype(BF16), upper)
    slot_c = [
        4.0 * r_col[k][:, :1] + jnp.sum(before_c * hit_c[k], axis=1, keepdims=True) for k in range(2)
    ]
    slot_r = [
        4.0 * r_row[k][:1, :] + jnp.sum(before_r * hit_r[k], axis=0, keepdims=True) for k in range(2)
    ]
    row = iota((1024, 128), 0)
    row_slot = (4 * expert_of(row >> 3) + (row & 3)).astype(F32)
    row_half = (row >> 2) & 1
    chosen = (row_slot == slot_r[0]) | (row_slot == slot_r[1])
    for g in range(2):
        disp[:, g * 128 : (g + 1) * 128] = jnp.where(chosen & (row_half == g), 1.0, 0.0).astype(BF16)
    col = iota((TOK, 1024), 1)
    col_slot = (4 * expert_of(col >> 3) + (col & 3)).astype(F32)
    col_half = (col >> 2) & 1
    for k in range(2):
        for g in range(2):
            at = (2 * k + g) * 128
            pick[at : at + 128, :] = jnp.where(
                (col_slot == slot_c[k]) & (col_half == g), 1.0, 0.0
            ).astype(BF16)
    share_sum = ish_ref[0:1, :] + ish_ref[1:2, :]
    for k in range(2):
        weight = gw_ref[...] * ish_ref[k : k + 1, :] / share_sum
        wts[k] = jnp.broadcast_to(weight, (128, TOK)).T
    p_o, p_i = iota((256, 256), 0), iota((256, 256), 1)
    perm[0] = jnp.where(
        p_i == 8 * ((p_o >> 2) & 31) + 4 * (p_o >> 7) + (p_o & 3), 1.0, 0.0
    ).astype(BF16)
    perm[1] = jnp.where(
        p_o == 8 * ((p_i >> 2) & 31) + 4 * (p_i >> 7) + (p_i & 3), 1.0, 0.0
    ).astype(BF16)

    def normed_heads(ten, at, size, gain_ref):
        rows = qkv_r[ten, at : at + size, :].astype(F32)
        square = rows * rows
        first = iota((size, 128), 1) < HD
        sum0 = jnp.sum(jnp.where(first, square, 0.0), axis=1, keepdims=True)
        sum1 = jnp.sum(jnp.where(first, 0.0, square), axis=1, keepdims=True)
        factor = jnp.where(
            first, lax.rsqrt(sum0 * (1.0 / HD) + EPS), lax.rsqrt(sum1 * (1.0 / HD) + EPS)
        )
        gain = jnp.concatenate([gain_ref[...]] * 2, axis=1)
        return (rows * factor * gain).astype(BF16).astype(F32)

    drain(qkv_r.at[0, pl.ds(0, 15 * TOK)], qkv_recv.at[0])
    step = 512
    for at in range(0, SEQ, step):
        turned = normed_heads(0, at, step, kg_ref).T
        sub = iota((128, step), 0)
        for h in range(2):
            bias = fc_ref[h : h + 1, at : at + step]
            high = bias.astype(BF16).astype(F32)
            middle = (bias - high).astype(BF16).astype(F32)
            low = bias - high - middle
            base = 64 * (1 - h)
            extra = jnp.where(
                sub == base, high, jnp.where(sub == base + 1, middle, jnp.where(sub == base + 2, low, 0.0))
            )
            mine = (sub < HD) if h == 0 else (sub >= HD)
            kt[h, :, at : at + step] = jnp.where(mine, turned, extra).astype(BF16)
    drain(qkv_r.at[1, pl.ds(0, 15 * TOK)], qkv_recv.at[1])
    for at in range(0, SEQ, step):
        scaled = normed_heads(1, at, step, qg_ref) * (HD**-0.5)
        lane = iota((step, 128), 1)
        for h in range(2):
            base = 64 * (1 - h)
            mine = (lane < HD) if h == 0 else (lane >= HD)
            extra = jnp.where((lane >= base) & (lane < base + 3), -1.0, 0.0)
            qh[h, at : at + step, :] = jnp.where(mine, scaled, extra).astype(BF16)

    drain(wr.at[pl.ds(0, 512), pl.ds(0, 1024)], w_near.at[0])
    def relay(start, ssem, rsem):
        for s, (near, onward) in enumerate(((3, 1), (1, 3))):
            part = wr.at[
                pl.ds(pl.multiple_of(start + 256 * s, 256), 256),
                pl.ds(pl.multiple_of(mod(y + near, 4) * 512, 512), 512),
            ]
            remote(part, part, ssem, rsem, (sp, mod(y + onward, 4) * 2 + c)).start()

    relay(512 * parity, w_send.at[2], w_far.at[0])
    across = (
        z * 4 + mod(x + 1, 4), z * 4 + mod(x + 3, 4), mod(z + 1, 4) * 4 + x, mod(z + 3, 4) * 4 + x
    )

    for step in (1, 3):
        for q, t in enumerate(across):
            part = wr.at[
                pl.ds(pl.multiple_of(512 * parity + 256 + 64 * q, 64), 64),
                pl.ds(pl.multiple_of(mod(y + step, 4) * 512, 512), 512),
            ]
            remote(part, part, w_send.at[5], w_near.at[2], (t, dp)).start()

    half = sp // 8
    a_cols = pl.ds(pl.multiple_of(mod(sp, 8) * 128, 128), 128)
    a_rows = pl.ds(pl.multiple_of(c * TOK, TOK), TOK)

    def return_block(i):
        for t in (2 * i, 2 * i + 1):
            own = jnp.logical_and(sp == t, half == c)
            rows = pl.ds(pl.multiple_of(t * TOK, TOK), TOK)

            @pl.when(own)
            def _(rows=rows):
                ar[a_rows, a_cols] = ao[rows, :]

            @pl.when(jnp.logical_not(own))
            def _(rows=rows, t=t):
                remote(ao.at[rows], ar.at[a_rows, a_cols], a_send, a_recv, (t, y * 2 + half)).start()

    blocks = SEQ // QB
    tri = iota((QB, QB), 1) <= iota((QB, QB), 0)
    first = iota((QB, 128), 1) < HD

    def weigh(i):
        at, keys = i * QB, (i + 1) * QB
        inverse = []
        for h in range(2):
            query = qh[h, at:keys, :]
            diag = jnp.where(tri, dot(query, kt[h, :, at:keys]), -jnp.inf)
            highest = jnp.max(diag, axis=1, keepdims=True)
            if at:
                past = dot(query, kt[h, :, :at])
                highest = jnp.maximum(highest, jnp.max(past, axis=1, keepdims=True))
            diag = jnp.exp(diag - highest)
            total = jnp.sum(diag, axis=1, keepdims=True)
            tile = i * (i + 1) // 2
            probs[h, tile + i] = diag.astype(BF16)
            if at:
                past = jnp.exp(past - highest)
                total = total + jnp.sum(past, axis=1, keepdims=True)
                for j in range(i):
                    probs[h, tile + j] = past[:, j * QB : (j + 1) * QB].astype(BF16)
            inverse.append(1.0 / total)
        scale[at:keys, :] = jnp.where(first, inverse[0], inverse[1])

    def combine(i):
        at, keys = i * QB, (i + 1) * QB
        results = []
        for h in range(2):
            result = None
            for j in range(i + 1):
                term = dot(probs[h, i * (i + 1) // 2 + j], qkv_r[2, j * QB : (j + 1) * QB, :])
                result = term if result is None else result + term
            results.append(result)
        ao[at:keys, :] = (jnp.where(first, results[0], results[1]) * scale[at:keys, :]).astype(BF16)

    def block_of(n):
        m = mod(n + sp // 2, blocks)
        odd = mod(m, 2)
        return (1 - odd) * (blocks - 1 - m // 2) + odd * (m // 2)

    for i in range(blocks):
        weigh(i)
    drain(qkv_r.at[2, pl.ds(0, 15 * TOK)], qkv_recv.at[2])

    def one_block(n, _):
        for i in range(blocks):
            pl.when(block_of(n) == i)(functools.partial(combine, i))
        return_block(block_of(n))

        @pl.when(n == 1)
        def _():
            drain(wr.at[pl.ds(0, 256), pl.ds(0, 1024)], w_near.at[1])
            drain(wr.at[pl.ds(0, 256), pl.ds(0, 1024)], w_near.at[2])
            relay(512 * (1 - parity), w_send.at[3], w_far.at[1])

        return 0

    lax.fori_loop(0, blocks, one_block, 0)

    local[3].wait()
    local[4].wait()
    drain(wr.at[:, pl.ds(0, 256)], w_part)
    drain(wr.at[pl.ds(0, 512), pl.ds(0, 512)], w_far.at[0])
    drain(wr.at[pl.ds(0, 512), pl.ds(0, 512)], w_far.at[1])
    own_in = half == c

    @pl.when(own_in)
    def _():
        drain(ao.at[pl.ds(0, 15 * TOK)], a_recv)
        drain(ao.at[pl.ds(0, 15 * TOK)], a_send)

    @pl.when(jnp.logical_not(own_in))
    def _():
        drain(ao.at[pl.ds(0, 16 * TOK)], a_recv)
        drain(ao.at[pl.ds(0, 16 * TOK)], a_send)

    other = ar[pl.ds(pl.multiple_of((1 - c) * TOK, TOK), TOK), :]
    for n in range(4):
        cols = pl.ds(512 * n, 512)
        psend[n] = dot(other, wr[:, cols])
        remote(psend.at[n], precv.at[n], p_send, p_recv, (sp, y * 2 + 1 - c)).start()
    mine = ar[a_rows, :]
    parts = [dot(mine, wr[:, 512 * n : 512 * n + 512]) for n in range(4)]
    drain(precv, p_recv)
    mids = []
    square = None
    for n in range(4):
        cols = slice(512 * n, 512 * n + 512)
        mid = (resid_s[:, cols].astype(F32) + (parts[n] + precv[n])).astype(BF16)
        resid_s[:, cols] = mid
        mid = mid.astype(F32)
        mids.append(mid)
        term = jnp.sum(mid * mid, axis=1, keepdims=True)
        square = term if square is None else square + term
    factor = lax.rsqrt(square * (1.0 / D) + EPS)
    normed = [
        (mids[n] * factor * ng_ref[:, 512 * n : 512 * n + 512]).astype(BF16) for n in range(4)
    ]
    halves = [jnp.concatenate(normed[2 * g : 2 * g + 2], axis=1) for g in range(2)]
    stacked = jnp.concatenate(halves, axis=0)
    pl.semaphore_wait(ready, 7)

    def partner(i, way):
        d = mod(MULT * i, 128)
        dz, dx, dy, dc = mod(d, 4), mod(d // 4, 4), mod(d // 16, 4), d // 64
        ts = mod(z + way * dz + 4, 4) * 4 + mod(x + way * dx + 4, 4)
        td = mod(y + way * dy + 4, 4) * 2 + mod(c + dc, 2)
        return ts, td

    def send_rows(i, _):
        remote(send.at[i], recv.at[i], d_send, d_recv.at[i // 32], partner(i, sign)).start()
        return 0

    for b in range(4):
        send[b * 32 : (b + 1) * 32] = (
            dot(disp[b * 256 : (b + 1) * 256, :], stacked).astype(BF16).reshape(32, 8, 1024)
        )
        lax.fori_loop(max(1, b * 32), b * 32 + 32, send_rows, 0)
    recv[0] = send[0]
    for copy in experts:
        copy.wait()

    def wait_block(ref, sem, b):
        @pl.when(b == 0)
        def _():
            drain(ref.at[pl.ds(0, 31)], sem.at[b])

        @pl.when(b > 0)
        def _():
            drain(ref.at[pl.ds(0, 32)], sem.at[b])

    def run_expert(b, _):
        wait_block(recv, d_recv, b)
        at = pl.multiple_of(b * 32, 32)
        rows = recv[pl.ds(at, 32)].reshape(256, 1024)
        rows = dot(perm[0], rows).astype(BF16)
        gate = dot(rows[:128], wg[:1024, :]) + dot(rows[128:], wg[1024:, :])
        up = dot(rows[:128], wu[:1024, :]) + dot(rows[128:], wu[1024:, :])
        hidden = (gate / (1.0 + jnp.exp(-gate)) * up).astype(BF16)
        result = [dot(hidden, wd[:, g * 1024 : (g + 1) * 1024]).astype(BF16) for g in range(2)]
        back = dot(perm[1], jnp.concatenate(result, axis=0)).astype(BF16)
        ysend[pl.ds(at, 32)] = back.reshape(32, 8, 1024)

        def send_back(i, _):
            d = mod(MULT * i, 128)
            src_sign = sign * (1 - 2 * (d // 64))
            remote(ysend.at[i], ret.at[i], r_send, r_recv.at[b], partner(i, -src_sign)).start()
            return 0

        lax.fori_loop(jnp.where(b == 0, 1, b * 32), b * 32 + 32, send_back, 0)

        @pl.when(b == 0)
        def _():
            ret[0] = ysend[0]

        return 0

    lax.fori_loop(0, 4, run_expert, 0)
    def collect(b, _):
        wait_block(ret, r_recv, b)
        rows = ret[pl.ds(pl.multiple_of(b * 32, 32), 32)].reshape(256, 1024)
        picked = dot(pick[:, pl.ds(pl.multiple_of(b * 256, 256), 256)], rows)

        @pl.when(b == 0)
        def _():
            acc[...] = picked

        @pl.when(b > 0)
        def _():
            acc[...] += picked

        return 0

    lax.fori_loop(0, 4, collect, 0)
    for g in range(2):
        cols = slice(1024 * g, 1024 * g + 1024)
        mixed = wts[0][:, :1] * acc[g * 128 : g * 128 + 128, :]
        mixed = mixed + wts[1][:, :1] * acc[(2 + g) * 128 : (3 + g) * 128, :]
        out_ref[:, cols] = (resid_s[:, cols].astype(F32) + mixed).astype(BF16)

    for ten in range(3):
        drain(qkv_r.at[ten, pl.ds(0, 15 * TOK)], qkv_send.at[ten])
    drain(wr.at[pl.ds(0, 512), pl.ds(0, 1024)], w_send.at[0])
    drain(wr.at[:, pl.ds(0, 256)], w_send.at[1])
    drain(wr.at[pl.ds(0, 512), pl.ds(0, 512)], w_send.at[2])
    drain(wr.at[pl.ds(0, 512), pl.ds(0, 512)], w_send.at[3])
    drain(wr.at[pl.ds(0, 256), pl.ds(0, 1024)], w_send.at[4])
    drain(wr.at[pl.ds(0, 256), pl.ds(0, 1024)], w_send.at[5])
    drain(precv, p_send)
    drain(recv.at[pl.ds(0, 127)], d_send)
    drain(recv.at[pl.ds(0, 127)], r_send)


def shards(
    resid,
    queries,
    keys,
    values,
    forget_cache,
    query_gain,
    key_gain,
    out_weight,
    norm_gain,
    routes,
    group_weight,
    inner_share,
    expert_gate,
    expert_up,
    expert_down,
):
    hbm_spec = pl.BlockSpec(memory_space=pltpu.HBM)
    vmem_spec = pl.BlockSpec(memory_space=pltpu.VMEM)
    vm = pltpu.VMEM
    dma = pltpu.SemaphoreType.DMA
    out = pl.pallas_call(
        kernel,
        out_shape=jax.ShapeDtypeStruct((TOK, D), BF16),
        in_specs=[hbm_spec] * 15,
        out_specs=vmem_spec,
        scratch_shapes=[
            vm((2, SEQ), F32),
            vm((1, HD), F32),
            vm((1, HD), F32),
            vm((1, D), F32),
            vm((2, TOK), jnp.int32),
            vm((1, TOK), F32),
            vm((2, TOK), F32),
            vm((3, TOK, D), BF16),
            vm((3, SEQ, 128), BF16),
            vm((2, SEQ, 128), BF16),
            vm((2, 128, SEQ), BF16),
            vm((SEQ, 128), BF16),
            vm((2 * TOK, 1024), BF16),
            vm((2, 36, QB, QB), BF16),
            vm((SEQ, 128), F32),
            vm((1024, D), BF16),
            vm((4, TOK, 512), F32),
            vm((4, TOK, 512), F32),
            vm((TOK, D), BF16),
            vm((1024, 256), BF16),
            vm((512, 1024), BF16),
            vm((2, 256, 256), BF16),
            vm((D, FF), BF16),
            vm((D, FF), BF16),
            vm((FF, D), BF16),
            vm((128, 8, 1024), BF16),
            vm((128, 8, 1024), BF16),
            vm((128, 8, 1024), BF16),
            vm((128, 8, 1024), BF16),
            vm((512, 1024), F32),
            vm((2, TOK, 128), F32),
            dma((15,)),
            dma((3,)),
            dma((3,)),
            dma((6,)),
            dma((3,)),
            dma((2,)),
            dma,
            dma,
            dma,
            dma,
            dma,
            dma,
            dma((4,)),
            dma,
            dma((4,)),
            pltpu.SemaphoreType.REGULAR,
        ],
        compiler_params=pltpu.CompilerParams(
            collective_id=0, has_side_effects=True, vmem_limit_bytes=53 * 2**20
        ),
        name="layer",
    )(
        *[
            pltpu.with_memory_space_constraint(a, pltpu.HBM)
            for a in (
                queries[0],
                keys[0],
                values[0],
                resid[0],
                out_weight,
                expert_gate[0],
                expert_up[0],
                expert_down[0],
                forget_cache[0],
                query_gain.reshape(1, HD),
                key_gain.reshape(1, HD),
                norm_gain.reshape(1, D),
                routes[0].T,
                group_weight,
                inner_share[0].T,
            )
        ]
    )
    return out[None]


def solution(mesh):
    return jax.shard_map(
        shards,
        mesh=mesh,
        in_specs=(
            P("dp", "sp", None),
            P("dp", "sp", None),
            P("dp", "sp", None),
            P("dp", "sp", None),
            P("dp", "sp", None),
            P(),
            P(),
            P(None, "dp"),
            P(),
            P("dp", "sp", None),
            P("dp", "sp"),
            P("dp", "sp", None),
            P(("sp", "dp"), None, None),
            P(("sp", "dp"), None, None),
            P(("sp", "dp"), None, None),
        ),
        out_specs=P("dp", "sp", None),
        check_vma=False,
    )
```
